512 devices in a mesh: sp: 64 (over z, y), tp: 8 (over x, core).
Axes of the slice: x: 4, y: 8, z: 8, core: 2. Of those that a mesh axis runs over, the one named last changes fastest.
Arguments:
- tokens: bfloat16 [24576, 2048], P('sp', 'tp'), may hold values from -60 to 60
- pre_gain: bfloat16 [2048], P('tp'), may hold values from 0.099609375 to 1.8984375
- w_query: bfloat16 [2048, 1024], P('sp', 'tp'), may hold values from -1 to 1
- w_key: bfloat16 [2048, 1024], P('sp', 'tp'), may hold values from -1 to 1
- w_value: bfloat16 [2048, 1024], P('sp', 'tp'), may hold values from -0.125 to 0.125
- w_pool: bfloat16 [2048, 1024], P('sp', 'tp'), may hold values from -0.125 to 0.125
- lambdas: float32 [8], P('tp'), may hold values from 0.3 to 0.8
- sub_gain: float32 [128], replicated, may hold values from 0.1 to 1.9
- group_weight: bfloat16 [8, 128, 128], P('tp'), may hold values from -0.5 to 0.5
- pool_scale: float32 [1024], P('tp'), may hold values from 0.1 to 1.9
- w_out: bfloat16 [2048, 2048], P('tp', 'sp'), may hold values from -0.125 to 0.125
Outputs:
- mixed_out: bfloat16 [24576, 2048], P(('sp', 'tp'))
The draws below stay inside these ranges and needn't reach their ends.
All inputs are finite; a program needn't handle non-finite values.
Results may differ from the reference program's by a relative error of at most 0.015.
Values may be sent and summed in bfloat16 or wider, within the bound.
A program may use at most 128 MiB of HBM per device.

```python
import math
import jax
import jax.numpy as jnp
import numpy as np
from jax import lax

D = 2048
HEADS = 8
HDIM = 64
VDIM = 128
GROUPS = 8
GDIM = 128
TOKENS = 24576


def draw_tokens(key, part):
    noise = jax.random.normal(jax.random.fold_in(key, 11), (TOKENS, D), jnp.float32)
    row_scale = jnp.exp(jax.random.uniform(jax.random.fold_in(key, 12), (TOKENS, 1), jnp.float32, 0.0, math.log(10.0)))
    column_rise = 1.1 * jnp.arange(D, dtype=jnp.float32)[None, :] / D
    column_scale = jnp.exp(jax.random.uniform(jax.random.fold_in(key, 13), (1, D), jnp.float32, -0.7, 0.7) + column_rise)
    result = noise * row_scale * column_scale
    return jnp.clip(result, -60.0, 60.0).astype(jnp.bfloat16)


def query_key_pair(key):
    columns = HEADS * 2 * HDIM
    spread = math.sqrt(2.0 / D)
    first = jax.random.normal(jax.random.fold_in(key, 21), (D, columns), jnp.float32) * spread
    second = jax.random.normal(jax.random.fold_in(key, 22), (D, columns), jnp.float32) * spread
    return (jnp.clip(first, -1.0, 1.0), jnp.clip(second, -1.0, 1.0))


def draw_w_query(key, part):
    return query_key_pair(key)[0].astype(jnp.bfloat16)


def draw_w_key(key, part):
    return query_key_pair(key)[1].astype(jnp.bfloat16)


def level_of(rng, shape, split, least, high):
    factor_of, own = 1.0, jax.random.fold_in(rng, 6)
    for dim, shards_of in split:
        heights = jnp.exp(jax.random.uniform(jax.random.fold_in(own, dim), (shards_of,), jnp.float32, least / len(split), high / len(split)))
        factor_of = factor_of * jnp.repeat(heights, shape[dim] // shards_of).reshape([-1 if axis == dim else 1 for axis in range(len(shape))])
    return factor_of


def bell_draw(stream_key, extent, width, reach, shards=(), held_as=jnp.bfloat16):
    values = jax.random.normal(stream_key, extent, jnp.float32) * width
    if len(shards) > 0:
        values = level_of(stream_key, extent, shards, -0.22, 0.18) * values
    return jnp.clip(values, min=-reach, max=reach).astype(held_as)


def setup_inputs(seed: int = 0) -> dict:
    splits = jax.random.split(jax.random.key(seed), 12)
    tokens = draw_tokens(jax.random.fold_in(splits[11], 71), 0)
    pre_gain = jnp.clip(1.0 + 0.18 * jax.random.normal(splits[1], (D,), jnp.float32), 0.099609375, 1.8984375).astype(jnp.bfloat16)
    w_query = draw_w_query(jax.random.fold_in(splits[11], 71), 0)
    w_key = draw_w_key(jax.random.fold_in(splits[11], 71), 0)
    w_value = bell_draw(splits[4], (D, HEADS * VDIM), D ** -0.5, 0.125, ((0, 64), (1, 8)))
    w_pool = bell_draw(splits[5], (D, GROUPS * GDIM), D ** -0.5, 0.125, ((0, 64), (1, 8)))
    lambdas = jnp.clip(0.3 + 0.5 * jax.random.uniform(splits[6], (HEADS,), jnp.float32) ** level_of(splits[6], (HEADS,), ((0, 8),), -0.2, 0.2), 0.3, 0.8)
    sub_gain = jnp.clip(1.0 + 0.18 * jax.random.normal(splits[7], (VDIM,), jnp.float32), 0.1, 1.9)
    group_weight = bell_draw(splits[8], (GROUPS, GDIM, GDIM), GDIM ** -0.5, 0.5, ((0, 8),))
    pool_scale = jnp.clip(1.0 + 0.18 * jax.random.normal(splits[9], (GROUPS * GDIM,), jnp.float32), 0.1, 1.9)
    w_out = bell_draw(splits[10], (HEADS * (VDIM + GDIM), D), (HEADS * (VDIM + GDIM)) ** -0.5, 0.125, ((0, 8), (1, 64)))
    return {"tokens": tokens, "pre_gain": pre_gain, "w_query": w_query, "w_key": w_key, "w_value": w_value, "w_pool": w_pool, "lambdas": lambdas, "sub_gain": sub_gain, "group_weight": group_weight, "pool_scale": pool_scale, "w_out": w_out}


EPSILON = 1e-06
WINDOWS = (2, 4, 8, 16)
RIM_ROWS = 15

def head_block(query_head, key_head, value_head, weight_two, first_row):
    block_len = query_head.shape[0]
    key_len = key_head.shape[0]
    score_scale = 1.0 / math.sqrt(HDIM)
    scores = jnp.einsum('qmd,kmd->mqk', query_head.astype(jnp.float32), key_head.astype(jnp.float32)) * score_scale
    allowed = jnp.arange(key_len, dtype=jnp.int32)[None, :] <= (first_row + jnp.arange(block_len, dtype=jnp.int32))[:, None]
    scores = jnp.where(allowed[None], scores, -jnp.inf)
    row_max = lax.optimization_barrier(jnp.max(scores, axis=-1, keepdims=True))
    expo = jnp.where(allowed[None], jnp.exp(scores - row_max), 0.0)
    row_sum = lax.optimization_barrier(jnp.sum(expo, axis=-1))
    rounded = lax.optimization_barrier(expo.astype(jnp.bfloat16)).astype(jnp.float32)
    weighted = jnp.einsum('mqk,kd->mqd', rounded, value_head.astype(jnp.float32))
    head_mix = weighted[0] / row_sum[0][:, None] - weight_two * weighted[1] / row_sum[1][:, None]
    return head_mix

def reference(tokens, pre_gain, w_query, w_key, w_value, w_pool, lambdas, sub_gain, group_weight, pool_scale, w_out):
    features = tokens.astype(jnp.float32)
    inverse = lax.rsqrt(lax.optimization_barrier(jnp.mean(features * features, axis=1, keepdims=True)) + EPSILON)
    scaled = (features * pre_gain.astype(jnp.float32)).astype(jnp.bfloat16)

    def project(weight):
        return (jnp.dot(scaled, weight, preferred_element_type=jnp.float32) * inverse).astype(jnp.bfloat16)
    queries = project(w_query).reshape(TOKENS, HEADS, 2, HDIM)
    key_rows = project(w_key).reshape(TOKENS, HEADS, 2, HDIM)
    values = project(w_value).reshape(TOKENS, HEADS, VDIM)
    pool_in = project(w_pool)
    block_len = math.gcd(TOKENS, 512)
    pieces = []
    for block_index in range(TOKENS // block_len):
        first_row = block_index * block_len
        key_len = first_row + block_len
        query_heads = jnp.transpose(queries[first_row:key_len], (1, 0, 2, 3))
        key_heads = jnp.transpose(key_rows[:key_len], (1, 0, 2, 3))
        value_heads = jnp.transpose(values[:key_len], (1, 0, 2))

        def one_head(packed):
            return head_block(packed[0], packed[1], packed[2], packed[3], first_row)
        mixed_heads = lax.map(one_head, (query_heads, key_heads, value_heads, lambdas))
        mean_sq = lax.optimization_barrier(jnp.mean(mixed_heads * mixed_heads, axis=-1, keepdims=True))
        normed = mixed_heads * lax.rsqrt(mean_sq + EPSILON) * sub_gain
        pieces.append(jnp.transpose(normed, (1, 0, 2)).astype(jnp.bfloat16))
    attention = jnp.concatenate(pieces, axis=0)
    pool_float = pool_in.astype(jnp.float32)
    extended = jnp.concatenate([jnp.zeros((RIM_ROWS, GROUPS * GDIM), jnp.float32), pool_float], axis=0)
    running = jnp.concatenate([jnp.zeros((1, GROUPS * GDIM), jnp.float32), jnp.cumsum(extended, axis=0)], axis=0)
    running_top = running[RIM_ROWS + 1:]
    positions = jnp.arange(TOKENS, dtype=jnp.int32)
    window_of_column = np.repeat(np.arange(GROUPS) % len(WINDOWS), GDIM)
    average = jnp.zeros_like(running_top)
    for window_slot, window_span in enumerate(WINDOWS):
        running_low = running[RIM_ROWS + 1 - window_span:RIM_ROWS + 1 - window_span + TOKENS]
        window_count = jnp.minimum(positions + 1, window_span).astype(jnp.float32)
        average = average + jnp.where(window_of_column[None, :] == window_slot, (running_top - running_low) / window_count[:, None], 0.0)
    differ = (average - pool_float).astype(jnp.bfloat16).reshape(TOKENS, GROUPS, GDIM)
    pooled = jnp.einsum('tgc,gcd->tgd', differ.astype(jnp.float32), group_weight.astype(jnp.float32))
    pooled = (pooled * pool_scale.reshape(GROUPS, GDIM)).astype(jnp.bfloat16)
    branch = jnp.concatenate([attention, pooled], axis=2).reshape(TOKENS, HEADS * (VDIM + GDIM))
    return jnp.dot(branch, w_out, preferred_element_type=jnp.float32).astype(jnp.bfloat16)
```

```python
import functools
import math

import jax
import jax.numpy as jnp
from jax import lax
from jax.experimental import pallas as pl
from jax.experimental.pallas import tpu as pltpu
from jax.sharding import PartitionSpec as P

MESH = pl.DeviceIdType.MESH
VMEM = pltpu.VMEM
EPSILON = 1e-06
NEG_LARGE = -1e30
F32, BF16 = jnp.float32, jnp.bfloat16
RIM = 16


def grid_of(sp):
    ny = 2 ** ((sp.bit_length() - 1) // 2)
    return sp // ny, ny


def vspec(n):
    return [pl.BlockSpec(memory_space=VMEM)] * n


def sds(*shape, dtype=BF16):
    return jax.ShapeDtypeStruct(shape, dtype)


def call(kernel, ins, outs, scratch=(), cid=None, limit=40 << 20, name=None, flops=1 << 24):
    params = dict(vmem_limit_bytes=limit)
    if cid is not None:
        params.update(collective_id=cid, has_side_effects=True)
    return pl.pallas_call(
        kernel,
        out_shape=tuple(outs),
        in_specs=vspec(len(ins)),
        out_specs=tuple(vspec(len(outs))),
        scratch_shapes=list(scratch),
        compiler_params=pltpu.CompilerParams(**params),
        cost_estimate=pl.CostEstimate(flops=flops, bytes_accessed=1 << 20, transcendentals=0),
        name=name,
    )(*ins)


def rcopy(src, dst, ssem, rsem, dev):
    return pltpu.make_async_remote_copy(
        src_ref=src, dst_ref=dst, send_sem=ssem, recv_sem=rsem, device_id=dev, device_id_type=MESH
    )


def greet(peers):
    barrier = pltpu.get_barrier_semaphore()
    for dev in peers:
        pl.semaphore_signal(barrier, inc=1, device_id=dev, device_id_type=MESH)
    pl.semaphore_wait(barrier, len(peers))


def hops(n, direction, sub):
    return n // 2 if (direction + sub) % 2 == 0 else (n - 1) // 2


class Ring:
    def __init__(self, n, me, dev, piece, subs, ssem, rsem):
        self.n, self.me, self.dev, self.piece, self.subs = n, me, dev, piece, subs
        self.ssem, self.rsem = ssem, rsem
        self.steps = n // 2

    def copy(self, d, sub, k):
        sign = 1 if d == 0 else -1
        block = (self.me - sign * k) % self.n
        ref = self.piece(block, sub)
        return rcopy(
            ref, ref, self.ssem.at[d, sub, k], self.rsem.at[d, sub, k], self.dev((self.me + sign) % self.n)
        )

    def step(self, k):
        for sub in range(self.subs):
            for d in range(2):
                if k > 0 and k - 1 < hops(self.n, d, sub):
                    self.copy(d, sub, k - 1).wait_recv()
                if k < hops(self.n, d, sub):
                    self.copy(d, sub, k).start()

    def finish(self):
        for k in range(self.steps):
            for sub in range(self.subs):
                for d in range(2):
                    if k < hops(self.n, d, sub):
                        self.copy(d, sub, k).wait_send()


def ring_sems(n, subs):
    return [pltpu.SemaphoreType.DMA((2, subs, n // 2)), pltpu.SemaphoreType.DMA((2, subs, n // 2))]


def gather_kernel(nz, ny, nx, tok_ref, w_ref, tok_full, w_full, ts, tr, ys, yr, zs, zr, as_, ar, bs, br):
    s, t = lax.axis_index("sp"), lax.axis_index("tp")
    z, y, x, c = s // ny, s % ny, t // 2, t % 2
    half = w_ref.shape[0] // 2
    partner = (s, x * 2 + 1 - c)
    across = [(s, ((x + d) % nx) * 2 + c) for d in range(1, nx)]
    along_y = [(z * ny + (y + d) % ny, t) for d in range(1, ny)]
    along_z = [(((z + d) % nz) * ny + y, t) for d in range(1, nz)]
    greet([partner] + across + along_y + along_z)

    ysends = [
        rcopy(w_ref.at[0:half], w_full.at[z, y, 0], ys.at[d], yr.at[d], along_y[d]) for d in range(ny - 1)
    ]
    zsends = [
        rcopy(w_ref.at[half:], w_full.at[z, y, 1], zs.at[d], zr.at[d], along_z[d]) for d in range(nz - 1)
    ]
    tsends = [rcopy(tok_ref, tok_full.at[t], ts.at[d], tr.at[d], across[d]) for d in range(nx - 1)]
    tsends.append(rcopy(tok_ref, tok_full.at[t], ts.at[nx - 1], tr.at[nx - 1], partner))
    for copy in ysends + zsends + tsends:
        copy.start()
    w_full[z, y, 0] = w_ref[0:half]
    w_full[z, y, 1] = w_ref[half:]
    tok_full[t] = tok_ref[...]

    def piece_a(block, sub):
        return w_full.at[block, sub * (ny // 2) : (sub + 1) * (ny // 2), 0]

    def piece_b(block, sub):
        return w_full.at[sub * (nz // 2) : (sub + 1) * (nz // 2), block, 1]

    ring_a = Ring(nz, z, lambda i: (i * ny + y, t), piece_a, 2, as_, ar)
    ring_b = Ring(ny, y, lambda i: (z * ny + i, t), piece_b, 2, bs, br)
    for copy in ysends:
        copy.wait_recv()
    ring_a.step(0)
    for copy in zsends:
        copy.wait_recv()
    ring_b.step(0)
    relays = []
    for k in range(1, max(ring_a.steps, ring_b.steps) + 1):
        if k <= ring_a.steps:
            ring_a.step(k)
        if k <= ring_b.steps:
            ring_b.step(k)
        if k == 1:
            for d in range(nx - 1):
                tsends[d].wait_recv()
                source = ((x - 1 - d) % nx) * 2 + c
                relays.append(
                    rcopy(tok_full.at[source], tok_full.at[source], ts.at[nx + d], tr.at[nx + d], partner)
                )
                relays[-1].start()
    tsends[-1].wait_recv()
    for copy in relays:
        copy.wait_recv()
    for copy in ysends + zsends + tsends + relays:
        copy.wait_send()
    ring_a.finish()
    ring_b.finish()


def project_kernel(tp, tok_ref, w_ref, qt_ref, k_ref, vt_ref, pool_ref, scaled, sq):
    rows, part = qt_ref.shape[1], tok_ref.shape[2]
    sq[...] = jnp.zeros_like(sq)
    for t in range(tp):
        x = tok_ref[t, 0:rows].astype(F32)
        gain = tok_ref[t, rows : rows + 1].astype(F32)
        squares = x * x
        for i in range(part // 128):
            sq[...] += squares[:, i * 128 : (i + 1) * 128]
        scaled[:, t * part : (t + 1) * part] = (x * gain).astype(BF16)
    inverse = lax.rsqrt(jnp.sum(sq[...], axis=1, keepdims=True) / (tp * part) + EPSILON)

    def project(at):
        out = jnp.dot(scaled[...], w_ref[:, at * 128 : at * 128 + 256], preferred_element_type=F32) * inverse
        return out[:, 0:128].astype(BF16), out[:, 128:256].astype(BF16)

    q, k = project(0)
    qt_ref[...] = jnp.transpose(q.astype(F32)).astype(BF16)
    k_ref[...] = k
    v, p = project(2)
    vt_ref[...] = jnp.transpose(v.astype(F32)).astype(BF16)
    pool_ref[...] = p


def spread_kernel(
    nz, ny, q_ref, k_ref, v_ref, p_ref, q_all, k_all, v_all, halo, zs, zr, ys, yr, hs, hr
):
    s, t = lax.axis_index("sp"), lax.axis_index("tp")
    z, y = s // ny, s % ny
    sp = nz * ny
    dev_z = lambda i: (i * ny + y, t)
    dev_y = lambda i: (z * ny + i, t)
    rows = p_ref.shape[0]
    nxt, prv = ((s + 1) % sp, t), ((s + sp - 1) % sp, t)
    peers = [dev_z((z + 1) % nz), dev_z((z + nz - 1) % nz), dev_y((y + 1) % ny), dev_y((y + ny - 1) % ny)]
    greet(peers + [nxt, prv])
    hcopy = rcopy(p_ref.at[rows - RIM :], halo, hs, hr, nxt)
    hcopy.start()
    q_all[y] = q_ref[...]
    k_all[z] = k_ref[...]
    v_all[z] = v_ref[...]
    qd = q_ref.shape[0] // 2
    ring_y = Ring(ny, y, dev_y, lambda b, i: q_all.at[b, i * qd : (i + 1) * qd], 2, ys, yr)
    ring_z = Ring(nz, z, dev_z, lambda b, i: (k_all if i == 0 else v_all).at[b], 2, zs, zr)
    for k in range(max(ring_y.steps, ring_z.steps) + 1):
        if k <= ring_z.steps:
            ring_z.step(k)
        if k <= ring_y.steps:
            ring_y.step(k)
    hcopy.wait_recv()
    hcopy.wait_send()
    ring_z.finish()
    ring_y.finish()


def attend_kernel(nz, ny, scale, q_all, k_all, v_all, acc_ref, st_ref):
    s = lax.axis_index("sp")
    z, y = s // ny, s % ny
    rows = q_all.shape[2]
    qd = q_all.shape[1] // 2
    vd = v_all.shape[1]
    lanes = 2 * rows
    width = min(256, rows)
    factor = scale / math.log(2.0)

    def chunk(yq, _):
        qt = q_all[yq]
        low = lax.broadcasted_iota(jnp.int32, qt.shape, 0) < qd
        zero = jnp.zeros_like(qt)
        qz = jnp.concatenate([jnp.where(low, qt, zero), jnp.where(low, zero, qt)], axis=1)
        st_ref[yq, 0:1] = jnp.full((1, lanes), NEG_LARGE, F32)
        st_ref[yq, 1:8] = jnp.zeros((7, lanes), F32)
        acc_ref[yq] = jnp.zeros((vd, lanes), F32)

        def pair(p, masked):
            keys = k_all[pl.ds(2 * p, 2)].reshape(2 * rows, 2 * qd)
            vals = jnp.concatenate([v_all[2 * p], v_all[2 * p + 1]], axis=1)
            for at in range(0, lanes, width):
                cols = slice(at, at + width)
                sc = jnp.dot(keys, qz[:, cols], preferred_element_type=F32)
                if masked:
                    lane = lax.broadcasted_iota(jnp.int32, (1, width), 1) + at
                    lane = jnp.where(lane >= rows, lane - rows, lane)
                    qpos = lane + (z * ny + yq) * rows
                    sub = lax.broadcasted_iota(jnp.int32, (2 * rows, 1), 0)
                    kpos = sub + (2 * p * ny + y) * rows
                    kpos = jnp.where(sub >= rows, kpos + (ny - 1) * rows, kpos)
                    allowed = kpos <= qpos
                    sc = jnp.where(allowed, sc, NEG_LARGE)
                old = st_ref[yq, 0:1, cols]
                new = jnp.maximum(old, jnp.max(sc, axis=0, keepdims=True))
                expo = jnp.exp2((sc - new) * factor)
                if masked:
                    expo = jnp.where(allowed, expo, 0.0)
                shrink = jnp.exp2((old - new) * factor)
                st_ref[yq, 0:1, cols] = new
                st_ref[yq, 1:2, cols] = st_ref[yq, 1:2, cols] * shrink + jnp.sum(expo, axis=0, keepdims=True)
                acc_ref[yq, :, cols] = acc_ref[yq, :, cols] * shrink + jnp.dot(
                    vals, expo.astype(BF16), preferred_element_type=F32
                )

        def full(p, carry):
            pair(p, False)
            return carry

        lax.fori_loop(0, z // 2, full, 0)

        @pl.when(jnp.logical_or(z % 2 == 1, yq >= y))
        def _():
            pair(z // 2, True)

        return 0

    lax.fori_loop(0, ny, chunk, 0)


def merge_kernel(ny, scale, acc_ref, st_ref, lam_ref, gain_ref, att_ref, mix, wbuf, sbuf, wland, sland, ws, wr, ss, sr):
    s, t = lax.axis_index("sp"), lax.axis_index("tp")
    z, y = s // ny, s % ny
    rows = att_ref.shape[0]
    factor = scale / math.log(2.0)
    dev = lambda i: (z * ny + i % ny, t)
    greet([dev(y + 1), dev(y + ny - 1)])

    def own(block, m):
        cols = slice(m * rows, (m + 1) * rows)
        return acc_ref[block, :, cols], st_ref[block, 0:1, cols], st_ref[block, 1:2, cols]

    def joined(a, b):
        top = jnp.maximum(a[1], b[1])
        fa, fb = jnp.exp2((a[1] - top) * factor), jnp.exp2((b[1] - top) * factor)
        return a[0] * fa + b[0] * fb, top, a[2] * fa + b[2] * fb

    def landed(d, m, k):
        return wland[d, m, k].astype(F32), sland[d, m, k, 0:1], sland[d, m, k, 1:2]

    def copies(d, m, k):
        to = dev(y + (1 if d == 0 else ny - 1))
        return [
            rcopy(wbuf.at[d, m, k], wland.at[d, m, k], ws.at[d, m, k], wr.at[d, m, k], to),
            rcopy(sbuf.at[d, m, k], sland.at[d, m, k], ss.at[d, m, k], sr.at[d, m, k], to),
        ]

    for k in range(ny // 2):
        for m in range(2):
            for d in range(2):
                n = hops(ny, d, m)
                if k >= n:
                    continue
                sign = 1 if d == 0 else -1
                block = (y + sign * (n - k)) % ny
                state = own(block, m)
                if k > 0:
                    for copy in copies(d, m, k - 1):
                        copy.wait_recv()
                    state = joined(state, landed(d, m, k - 1))
                wbuf[d, m, k] = state[0].astype(BF16)
                sbuf[d, m, k, 0:1] = state[1]
                sbuf[d, m, k, 1:2] = state[2]
                for copy in copies(d, m, k):
                    copy.start()
    for m in range(2):
        state = own(y, m)
        for d in range(2):
            n = hops(ny, d, m)
            if n > 0:
                for copy in copies(d, m, n - 1):
                    copy.wait_recv()
                state = joined(state, landed(d, m, n - 1))
        if m == 0:
            mix[...] = state[0] / state[2]
        else:
            mix[...] = mix[...] - lam_ref[0:1, 0:1] * state[0] / state[2]
    head = mix[...]
    mean = jnp.mean(head * head, axis=0, keepdims=True)
    normed = jnp.transpose(head * lax.rsqrt(mean + EPSILON)) * gain_ref[...]
    att_ref[...] = normed.astype(BF16)
    for k in range(ny // 2):
        for m in range(2):
            for d in range(2):
                if k < hops(ny, d, m):
                    for copy in copies(d, m, k):
                        copy.wait_send()


def output_kernel(p_ref, halo, gw_ref, ps_ref, att_ref, wo_ref, out_ref):
    s, t = lax.axis_index("sp"), lax.axis_index("tp")
    rows, dim = p_ref.shape
    here = p_ref[...].astype(F32)
    rim = jnp.where(s > 0, halo[...].astype(F32), 0.0)
    ext = jnp.concatenate([rim, here], axis=0)
    total = ext
    slot = t % 4
    for i in range(4):
        more = total + pltpu.roll(total, 1 << i, 0)
        total = jnp.where(i <= slot, more, total)
    span = jnp.where(slot == 0, 2, jnp.where(slot == 1, 4, jnp.where(slot == 2, 8, 16)))
    pos = s * rows + lax.broadcasted_iota(jnp.int32, (rows, 1), 0)
    count = jnp.minimum(pos + 1, span).astype(F32)
    differ = (total[RIM:] / count - here).astype(BF16)
    pooled = jnp.dot(differ, gw_ref[0], preferred_element_type=F32) * ps_ref[...]
    branch = jnp.concatenate([att_ref[...], pooled.astype(BF16)], axis=1)
    cols = wo_ref.shape[0]
    step = min(cols, 512)
    for at in range(0, cols, step):
        out_ref[:, at : at + step] = lax.dot_general(
            branch, wo_ref[at : at + step], (((1,), (1,)), ((), ())), preferred_element_type=F32
        ).astype(BF16)


def scatter_kernel(tp, part_ref, out_ref, land, ss, rs):
    s, t = lax.axis_index("sp"), lax.axis_index("tp")
    rows = out_ref.shape[0]
    peers = [(s, (t + d) % tp) for d in range(1, tp)]
    greet(peers)
    copies = []
    for d in range(1, tp):
        start = pl.multiple_of(((t + d) % tp) * rows, 16)
        copies.append(rcopy(part_ref.at[pl.ds(start, rows)], land.at[d - 1], ss.at[d - 1], rs.at[d - 1], peers[d - 1]))
        copies[-1].start()
    total = part_ref[pl.ds(pl.multiple_of(t * rows, 16), rows)].astype(F32)
    for d in range(1, tp):
        copies[d - 1].wait_recv()
        total = total + land[d - 1].astype(F32)
    out_ref[...] = total.astype(BF16)
    for copy in copies:
        copy.wait_send()


def local(sp, tp, tokens, pre_gain, w_query, w_key, w_value, w_pool, lambdas, sub_gain, group_weight, pool_scale, w_out):
    nz, ny = grid_of(sp)
    nx = tp // 2
    rows, part = tokens.shape
    wrows = w_query.shape[0]
    head = w_value.shape[1]
    qd = w_query.shape[1]
    wide = 2 * qd + 2 * head
    cols = w_out.shape[1]
    scale = 1.0 / math.sqrt(qd // 2)
    dma = pltpu.SemaphoreType.DMA
    tok = jnp.concatenate([tokens, jnp.broadcast_to(pre_gain[None], (16, part))], axis=0)
    wcat = jnp.concatenate([w_query, w_key, w_value, w_pool, w_out.T], axis=1)
    tok_full, w_full = call(
        functools.partial(gather_kernel, nz, ny, nx),
        (tok, wcat),
        (sds(tp, rows + 16, part), sds(nz, ny, 2, wrows // 2, wcat.shape[1])),
        [dma((2 * nx,)), dma((2 * nx,)), dma((ny,)), dma((ny,)), dma((nz,)), dma((nz,))]
        + ring_sems(nz, 2)
        + ring_sems(ny, 2),
        cid=0,
        name="gather",
    )
    w_all = w_full.reshape(sp * wrows, wcat.shape[1])
    qt, k, vt, pool = call(
        functools.partial(project_kernel, tp),
        (tok_full, w_all),
        (sds(qd, rows), sds(rows, qd), sds(head, rows), sds(rows, head)),
        [pltpu.VMEM((rows, tp * part), BF16), pltpu.VMEM((rows, 128), F32)],
        name="project",
    )
    q_all, k_all, v_all, halo = call(
        functools.partial(spread_kernel, nz, ny),
        (qt, k, vt, pool),
        (sds(ny, qd, rows), sds(nz, rows, qd), sds(nz, head, rows), sds(RIM, head)),
        ring_sems(nz, 2) + ring_sems(ny, 2) + [dma, dma],
        cid=1,
        name="spread",
    )
    acc, st = call(
        functools.partial(attend_kernel, nz, ny, scale),
        (q_all, k_all, v_all),
        (sds(ny, head, 2 * rows, dtype=F32), sds(ny, 8, 2 * rows, dtype=F32)),
        name="attend",
    )
    half = ny // 2
    (att,) = call(
        functools.partial(merge_kernel, ny, scale),
        (acc, st, jnp.broadcast_to(lambdas.reshape(1, 1), (8, 128)), sub_gain.reshape(1, head)),
        (sds(rows, head),),
        [
            pltpu.VMEM((head, rows), F32),
            pltpu.VMEM((2, 2, half, head, rows), BF16),
            pltpu.VMEM((2, 2, half, 8, rows), F32),
            pltpu.VMEM((2, 2, half, head, rows), BF16),
            pltpu.VMEM((2, 2, half, 8, rows), F32),
        ]
        + [dma((2, 2, half))] * 4,
        cid=2,
        name="merge",
    )
    (partial,) = call(
        output_kernel,
        (pool, halo, group_weight, pool_scale.reshape(1, head), att, w_all[:, wide:]),
        (sds(rows, sp * cols),),
        name="output",
    )
    out_rows = rows // tp
    (out,) = call(
        functools.partial(scatter_kernel, tp),
        (partial,),
        (sds(out_rows, sp * cols),),
        [pltpu.VMEM((tp - 1, out_rows, sp * cols), BF16), dma((tp - 1,)), dma((tp - 1,))],
        cid=3,
        name="scatter",
    )
    return out


def solution(mesh):
    placed = (
        P("sp", "tp"),
        P("tp"),
        P("sp", "tp"),
        P("sp", "tp"),
        P("sp", "tp"),
        P("sp", "tp"),
        P("tp"),
        P(),
        P("tp", None, None),
        P("tp"),
        P("tp", "sp"),
    )
    body = functools.partial(local, mesh.shape["sp"], mesh.shape["tp"])
    return jax.shard_map(body, mesh=mesh, in_specs=placed, out_specs=P(("sp", "tp"), None), check_vma=False)
```

```python
import functools
import math

import jax
import jax.numpy as jnp
from jax import lax
from jax.experimental import pallas as pl
from jax.experimental.pallas import tpu as pltpu
from jax.sharding import PartitionSpec as P

MESH = pl.DeviceIdType.MESH
VMEM = pltpu.VMEM
EPSILON = 1e-06
NEG_LARGE = -1e30
F32, BF16 = jnp.float32, jnp.bfloat16
RIM = 16
DEPTH = 256
LEAD = 3


def grid_of(sp):
    ny = 2 ** ((sp.bit_length() - 1) // 2)
    return sp // ny, ny


def vspec(n):
    return [pl.BlockSpec(memory_space=VMEM)] * n


def sds(*shape, dtype=BF16):
    return jax.ShapeDtypeStruct(shape, dtype)


def call(kernel, ins, outs, scratch=(), cid=None, limit=40 << 20, name=None, flops=1 << 24):
    params = dict(vmem_limit_bytes=limit)
    if cid is not None:
        params.update(collective_id=cid, has_side_effects=True)
    return pl.pallas_call(
        kernel,
        out_shape=tuple(outs),
        in_specs=vspec(len(ins)),
        out_specs=tuple(vspec(len(outs))),
        scratch_shapes=list(scratch),
        compiler_params=pltpu.CompilerParams(**params),
        cost_estimate=pl.CostEstimate(flops=flops, bytes_accessed=1 << 20, transcendentals=0),
        name=name,
    )(*ins)


def rcopy(src, dst, ssem, rsem, dev):
    return pltpu.make_async_remote_copy(
        src_ref=src, dst_ref=dst, send_sem=ssem, recv_sem=rsem, device_id=dev, device_id_type=MESH
    )


def greet(peers):
    barrier = pltpu.get_barrier_semaphore()
    for dev in peers:
        pl.semaphore_signal(barrier, inc=1, device_id=dev, device_id_type=MESH)
    pl.semaphore_wait(barrier, len(peers))


def hops(n, direction, sub):
    return n // 2 if (direction + sub) % 2 == 0 else (n - 1) // 2


class Ring:
    def __init__(self, n, me, dev, piece, subs, ssem, rsem):
        self.n, self.me, self.dev, self.piece, self.subs = n, me, dev, piece, subs
        self.ssem, self.rsem = ssem, rsem
        self.steps = n // 2

    def copy(self, d, sub, k):
        sign = 1 if d == 0 else -1
        block = (self.me - sign * k) % self.n
        ref = self.piece(block, sub)
        return rcopy(
            ref, ref, self.ssem.at[d, sub, k], self.rsem.at[d, sub, k], self.dev((self.me + sign) % self.n)
        )

    def step(self, k):
        for sub in range(self.subs):
            for d in range(2):
                if k > 0 and k - 1 < hops(self.n, d, sub):
                    self.copy(d, sub, k - 1).wait_recv()
                if k < hops(self.n, d, sub):
                    self.copy(d, sub, k).start()

    def finish(self):
        for k in range(self.steps):
            for sub in range(self.subs):
                for d in range(2):
                    if k < hops(self.n, d, sub):
                        self.copy(d, sub, k).wait_send()


def ring_sems(n, subs):
    return [pltpu.SemaphoreType.DMA((2, subs, n // 2)), pltpu.SemaphoreType.DMA((2, subs, n // 2))]


def gather_kernel(nz, ny, nx, tin_ref, gain_ref, wq_ref, wk_ref, wv_ref, wp_ref, tok_full, w_full, tok_ref, w_ref, ts, tr, ys, yr, zs, zr, as_, ar, bs, br):
    s, t = lax.axis_index("sp"), lax.axis_index("tp")
    z, y, x, c = s // ny, s % ny, t // 2, t % 2
    half = w_ref.shape[0] // 2
    rows = tin_ref.shape[0]
    tok_ref[0:rows] = tin_ref[...]
    tok_ref[rows:] = jnp.broadcast_to(gain_ref[...], (16, gain_ref.shape[1]))
    at = 0
    for ref in (wq_ref, wk_ref, wv_ref, wp_ref):
        w_ref[:, at : at + ref.shape[1]] = ref[...]
        at += ref.shape[1]
    partner = (s, x * 2 + 1 - c)
    across = [(s, ((x + d) % nx) * 2 + c) for d in range(1, nx)]
    along_y = [(z * ny + (y + d) % ny, t) for d in range(1, ny)]
    along_z = [(((z + d) % nz) * ny + y, t) for d in range(1, nz)]
    greet([partner] + across + along_y + along_z)

    ysends = [
        rcopy(w_ref.at[0:half], w_full.at[z, y, 0], ys.at[d], yr.at[d], along_y[d]) for d in range(ny - 1)
    ]
    zsends = [
        rcopy(w_ref.at[half:], w_full.at[z, y, 1], zs.at[d], zr.at[d], along_z[d]) for d in range(nz - 1)
    ]
    tsends = [rcopy(tok_ref, tok_full.at[t], ts.at[d], tr.at[d], across[d]) for d in range(nx - 1)]
    tsends.append(rcopy(tok_ref, tok_full.at[t], ts.at[nx - 1], tr.at[nx - 1], partner))
    for copy in ysends + zsends + tsends:
        copy.start()
    w_full[z, y, 0] = w_ref[0:half]
    w_full[z, y, 1] = w_ref[half:]
    tok_full[t] = tok_ref[...]

    def piece_a(block, sub):
        return w_full.at[block, sub * (ny // 2) : (sub + 1) * (ny // 2), 0]

    def piece_b(block, sub):
        return w_full.at[sub * (nz // 2) : (sub + 1) * (nz // 2), block, 1]

    ring_a = Ring(nz, z, lambda i: (i * ny + y, t), piece_a, 2, as_, ar)
    ring_b = Ring(ny, y, lambda i: (z * ny + i, t), piece_b, 2, bs, br)
    for copy in ysends:
        copy.wait_recv()
    ring_a.step(0)
    for copy in zsends:
        copy.wait_recv()
    ring_b.step(0)
    relays = []
    for k in range(1, max(ring_a.steps, ring_b.steps) + 1):
        if k <= ring_a.steps:
            ring_a.step(k)
        if k <= ring_b.steps:
            ring_b.step(k)
        if k == 1:
            for d in range(nx - 1):
                tsends[d].wait_recv()
                source = ((x - 1 - d) % nx) * 2 + c
                relays.append(
                    rcopy(tok_full.at[source], tok_full.at[source], ts.at[nx + d], tr.at[nx + d], partner)
                )
                relays[-1].start()
    tsends[-1].wait_recv()
    for copy in relays:
        copy.wait_recv()
    for copy in ysends + zsends + tsends + relays:
        copy.wait_send()
    ring_a.finish()
    ring_b.finish()


def project_kernel(tp, tok_ref, w_ref, qt_ref, k_ref, vt_ref, pool_ref, scaled, sq):
    rows, part = qt_ref.shape[1], tok_ref.shape[2]
    sq[...] = jnp.zeros_like(sq)
    for t in range(tp):
        x = tok_ref[t, 0:rows].astype(F32)
        gain = tok_ref[t, rows : rows + 1].astype(F32)
        squares = x * x
        for i in range(part // 128):
            sq[...] += squares[:, i * 128 : (i + 1) * 128]
        scaled[:, t * part : (t + 1) * part] = (x * gain).astype(BF16)
    inverse = lax.rsqrt(jnp.sum(sq[...], axis=1, keepdims=True) / (tp * part) + EPSILON)

    def project(at):
        out = jnp.dot(scaled[...], w_ref[:, at * 128 : at * 128 + 256], preferred_element_type=F32) * inverse
        return out[:, 0:128].astype(BF16), out[:, 128:256].astype(BF16)

    q, k = project(0)
    qt_ref[...] = jnp.transpose(q.astype(F32)).astype(BF16)
    k_ref[...] = k
    v, p = project(2)
    vt_ref[...] = jnp.transpose(v.astype(F32)).astype(BF16)
    pool_ref[...] = p


def spread_kernel(
    nz, ny, q_ref, k_ref, v_ref, p_ref, wo_ref, q_all, k_all, v_all, halo, wo_all, zs, zr, ys, yr, os, or_, ws, wr, hs, hr
):
    s, t = lax.axis_index("sp"), lax.axis_index("tp")
    z, y = s // ny, s % ny
    sp = nz * ny
    dev_z = lambda i: (i * ny + y, t)
    dev_y = lambda i: (z * ny + i, t)
    rows = p_ref.shape[0]
    nxt, prv = ((s + 1) % sp, t), ((s + sp - 1) % sp, t)
    along_z = [dev_z((z + d) % nz) for d in range(1, nz)]
    greet(along_z + [dev_y((y + 1) % ny), dev_y((y + ny - 1) % ny), nxt, prv])
    q_all[y] = q_ref[...]
    k_all[z] = k_ref[...]
    v_all[z] = v_ref[...]
    qd = q_ref.shape[0] // 2
    ring_y = Ring(ny, y, dev_y, lambda b, i: q_all.at[b, i * qd : (i + 1) * qd], 2, ys, yr)
    ring_z = Ring(nz, z, dev_z, lambda b, i: (k_all if i == 0 else v_all).at[b], 2, zs, zr)
    ring_z.step(0)
    ring_y.step(0)
    wcopies = [rcopy(wo_ref, wo_all.at[z, y], ws.at[d], wr.at[d], along_z[d]) for d in range(nz - 1)]
    hcopy = rcopy(p_ref.at[rows - RIM :], halo, hs, hr, nxt)
    for copy in wcopies + [hcopy]:
        copy.start()
    wo_all[z, y] = wo_ref[...]
    ring_o = Ring(ny, y, dev_y, lambda b, i: wo_all.at[i * (nz // 2) : (i + 1) * (nz // 2), b], 2, os, or_)
    for k in range(1, max(ring_y.steps, ring_z.steps) + 1):
        if k <= ring_z.steps:
            ring_z.step(k)
        if k <= ring_y.steps:
            ring_y.step(k)
        if k == 1:
            for copy in wcopies:
                copy.wait_recv()
            ring_o.step(0)
        elif k - 1 <= ring_o.steps:
            ring_o.step(k - 1)
    for k in range(max(ring_y.steps, ring_z.steps), ring_o.steps + 1):
        ring_o.step(k)
    hcopy.wait_recv()
    for copy in wcopies + [hcopy]:
        copy.wait_send()
    ring_z.finish()
    ring_y.finish()
    ring_o.finish()


def attend_kernel(nz, ny, scale, q_all, k_all, v_all, acc_ref, st_ref, qz_ref, bar_ref, sum_ref):
    s = lax.axis_index("sp")
    z, y = s // ny, s % ny
    rows = q_all.shape[2]
    qd = q_all.shape[1] // 2
    vd = v_all.shape[1]
    lanes = 2 * rows
    width = min(256, rows)
    factor = scale / math.log(2.0)

    def positions(yq, at, wide):
        lane = lax.broadcasted_iota(jnp.int32, (1, wide), 1) + at
        return jnp.where(lane >= rows, lane - rows, lane) + (z * ny + yq) * rows

    def set_queries(yq):
        qt = q_all[yq]
        low = lax.broadcasted_iota(jnp.int32, qt.shape, 0) < qd
        zero = jnp.zeros_like(qt)
        qz_ref[:, 0:rows] = jnp.where(low, qt, zero)
        qz_ref[:, rows:] = jnp.where(low, zero, qt)
        acc_ref[yq] = jnp.zeros((vd, lanes), F32)

    def tiles(yq, keys, vals, mask):
        depth = keys.shape[0] if keys.shape[0] == rows else min(DEPTH, rows)
        work = [(at, low) for at in range(0, lanes, width) for low in range(0, keys.shape[0], depth)]

        def scores(item):
            at, low = item
            return jnp.dot(keys[low : low + depth], qz_ref[:, at : at + width], preferred_element_type=F32)

        ahead = [scores(item) for item in work[:LEAD]]
        total, gain = None, None
        for i, (at, low) in enumerate(work):
            sc = ahead.pop(0)
            if i + LEAD < len(work):
                ahead.append(scores(work[i + LEAD]))
            cols = slice(at, at + width)
            expo = jnp.exp2(sc * factor - bar_ref[0:1, cols])
            if mask is not None:
                expo = jnp.where(mask(at)[low : low + depth], expo, 0.0)
            part = jnp.sum(expo.reshape(depth // 8, 8, width), axis=0)
            total = part if low == 0 else total + part
            term = jnp.dot(vals[:, low : low + depth], expo.astype(BF16), preferred_element_type=F32)
            gain = term if low == 0 else gain + term
            if low + depth == keys.shape[0]:
                sum_ref[:, cols] += total
                acc_ref[yq, :, cols] += gain

    def fast(yq, carry):
        st_ref[yq, 0:1] = jnp.full((1, lanes), NEG_LARGE, F32)
        st_ref[yq, 1:8] = jnp.zeros((7, lanes), F32)

        @pl.when(jnp.logical_or(z > 0, yq >= y))
        def _():
            set_queries(yq)
            few = min(128, rows)
            sc = jnp.dot(k_all[0, 0:few], qz_ref[...], preferred_element_type=F32)
            kpos = y * rows + lax.broadcasted_iota(jnp.int32, (few, 1), 0)
            bar = jnp.max(jnp.where(kpos <= positions(yq, 0, lanes), sc, NEG_LARGE), axis=0, keepdims=True)
            st_ref[yq, 0:1] = bar
            bar_ref[0:1] = bar * factor
            sum_ref[...] = jnp.zeros_like(sum_ref)

            def run(count, lo, hi):
                def body(b, carry):
                    first = lo + b * count
                    keys = k_all[pl.ds(first, count)].reshape(count * rows, 2 * qd)
                    vals = jnp.concatenate([v_all[first + i] for i in range(count)], axis=1)
                    tiles(yq, keys, vals, None)
                    return carry

                lax.fori_loop(0, (hi - lo) // count, body, 0)
                return lo + (hi - lo) // count * count

            blocks = z + jnp.where(yq > y, 1, 0)
            done = run(4, 0, blocks)
            done = run(2, done, blocks)
            run(1, done, blocks)

            @pl.when(yq == y)
            def _():
                kpos = (z * ny + y) * rows + lax.broadcasted_iota(jnp.int32, (rows, 1), 0)
                tiles(yq, k_all[z], v_all[z], lambda at: kpos <= positions(yq, at, width))

            st_ref[yq, 1:2] = jnp.sum(sum_ref[...], axis=0, keepdims=True)

        @pl.when(jnp.logical_and(z == 0, yq < y))
        def _():
            acc_ref[yq] = jnp.zeros((vd, lanes), F32)

        return carry

    lax.fori_loop(0, ny, fast, 0)
    largest = jnp.max(st_ref[:, 1:2])

    @pl.when(jnp.logical_not(largest < 2.0**80))
    def _():
        def slow(yq, carry):
            set_queries(yq)
            st_ref[yq, 0:1] = jnp.full((1, lanes), NEG_LARGE, F32)
            st_ref[yq, 1:8] = jnp.zeros((7, lanes), F32)

            def block(b, carry):
                kpos = (b * ny + y) * rows + lax.broadcasted_iota(jnp.int32, (rows, 1), 0)

                def group(g, carry):
                    at = pl.multiple_of(g * 128, 128)
                    cols = pl.ds(at, 128)
                    lane = lax.broadcasted_iota(jnp.int32, (1, 128), 1) + at
                    qpos = jnp.where(lane >= rows, lane - rows, lane) + (z * ny + yq) * rows
                    allowed = kpos <= qpos
                    sc = jnp.dot(k_all[b], qz_ref[:, cols], preferred_element_type=F32)
                    sc = jnp.where(allowed, sc, NEG_LARGE)
                    old = st_ref[yq, 0:1, cols]
                    new = jnp.maximum(old, jnp.max(sc, axis=0, keepdims=True))
                    expo = jnp.where(allowed, jnp.exp2((sc - new) * factor), 0.0)
                    shrink = jnp.exp2((old - new) * factor)
                    st_ref[yq, 0:1, cols] = new
                    st_ref[yq, 1:2, cols] = st_ref[yq, 1:2, cols] * shrink + jnp.sum(expo, axis=0, keepdims=True)
                    acc_ref[yq, :, cols] = acc_ref[yq, :, cols] * shrink + jnp.dot(
                        v_all[b], expo.astype(BF16), preferred_element_type=F32
                    )
                    return carry

                return lax.fori_loop(0, lanes // 128, group, carry)

            return lax.fori_loop(0, z + 1, block, carry)

        lax.fori_loop(0, ny, slow, 0)


def finish_kernel(
    ny, nx, scale, acc_ref, st_ref, lam_ref, gain_ref, p_ref, halo, gw_ref, ps_ref, wo_ref, out_ref,
    mix, branch, mine, wbuf, sbuf, wland, sland, give, take, send, land, ws, wr, ss, sr, gs, gr, os, or_,
):
    s, t = lax.axis_index("sp"), lax.axis_index("tp")
    z, y, x, c = s // ny, s % ny, t // 2, t % 2
    rows, head = p_ref.shape
    orows = out_ref.shape[0]
    chunks, _, width = mine.shape
    factor = scale / math.log(2.0)
    dev = lambda i: (z * ny + i % ny, t)
    partner = (s, x * 2 + 1 - c)
    across = [(s, ((x + d) % nx) * 2 + c) for d in range(1, nx)]
    greet([dev(y + 1), dev(y + ny - 1), partner] + across)

    def pooled():
        here = p_ref[...].astype(F32)
        rim = jnp.where(s > 0, halo[...].astype(F32), 0.0)
        total = jnp.concatenate([rim, here], axis=0)
        slot = t % 4
        for i in range(4):
            more = total + pltpu.roll(total, 1 << i, 0)
            total = jnp.where(i <= slot, more, total)
        span = jnp.where(slot == 0, 2, jnp.where(slot == 1, 4, jnp.where(slot == 2, 8, 16)))
        pos = s * rows + lax.broadcasted_iota(jnp.int32, (rows, 1), 0)
        count = jnp.minimum(pos + 1, span).astype(F32)
        differ = (total[RIM:] / count - here).astype(BF16)
        return (jnp.dot(differ, gw_ref[0], preferred_element_type=F32) * ps_ref[...]).astype(BF16)

    def own(block, m):
        cols = slice(m * rows, (m + 1) * rows)
        return acc_ref[block, :, cols], st_ref[block, 0:1, cols], st_ref[block, 1:2, cols]

    def joined(a, b):
        top = jnp.maximum(a[1], b[1])
        fa, fb = jnp.exp2((a[1] - top) * factor), jnp.exp2((b[1] - top) * factor)
        return a[0] * fa + b[0] * fb, top, a[2] * fa + b[2] * fb

    def landed(d, m, k):
        return wland[d, m, k].astype(F32), sland[d, m, k, 0:1], sland[d, m, k, 1:2]

    def copies(d, m, k):
        to = dev(y + (1 if d == 0 else ny - 1))
        return [
            rcopy(wbuf.at[d, m, k], wland.at[d, m, k], ws.at[d, m, k], wr.at[d, m, k], to),
            rcopy(sbuf.at[d, m, k], sland.at[d, m, k], ss.at[d, m, k], sr.at[d, m, k], to),
        ]

    for k in range(ny // 2):
        for m in range(2):
            for d in range(2):
                n = hops(ny, d, m)
                if k >= n:
                    continue
                sign = 1 if d == 0 else -1
                block = (y + sign * (n - k)) % ny
                state = own(block, m)
                if k > 0:
                    for copy in copies(d, m, k - 1):
                        copy.wait_recv()
                    state = joined(state, landed(d, m, k - 1))
                wbuf[d, m, k] = state[0].astype(BF16)
                sbuf[d, m, k, 0:1] = state[1]
                sbuf[d, m, k, 1:2] = state[2]
                for copy in copies(d, m, k):
                    copy.start()
        if k == 0:
            branch[:, head:] = pooled()
    for m in range(2):
        state = own(y, m)
        for d in range(2):
            n = hops(ny, d, m)
            if n > 0:
                for copy in copies(d, m, n - 1):
                    copy.wait_recv()
                state = joined(state, landed(d, m, n - 1))
        if m == 0:
            mix[...] = state[0] / state[2]
        else:
            mix[...] = mix[...] - lam_ref[0:1, 0:1] * state[0] / state[2]
    mixed = mix[...]
    mean = jnp.mean(mixed * mixed, axis=0, keepdims=True)
    normed = jnp.transpose(mixed * lax.rsqrt(mean + EPSILON)) * gain_ref[...]
    branch[:, 0:head] = normed.astype(BF16)

    def rows_of(core):
        starts = [pl.multiple_of((2 * i + core) * orows, 16) for i in range(nx)]
        return jnp.concatenate([branch[pl.ds(at, orows)] for at in starts], axis=0)

    def product(lhs, n):
        return lax.dot_general(
            lhs, wo_ref[n * width : (n + 1) * width], (((1,), (1,)), ((), ())), preferred_element_type=F32
        )

    lhs = rows_of(1 - c)
    gives = [rcopy(give.at[n], take.at[n], gs.at[n], gr.at[n], partner) for n in range(chunks)]
    for n in range(chunks):
        give[n] = product(lhs, n).astype(BF16)
        gives[n].start()
    lhs = rows_of(c)
    for n in range(chunks):
        mine[n] = product(lhs, n)
    outs = []
    for n in range(chunks):
        gives[n].wait_recv()
        both = mine[n] + take[n].astype(F32)
        mine[n] = both
        send[n] = both.astype(BF16)
        for d in range(1, nx):
            at = pl.multiple_of(((x + d) % nx) * orows, 16)
            outs.append(
                rcopy(send.at[n, pl.ds(at, orows)], land.at[d - 1, n], os.at[d - 1, n], or_.at[d - 1, n], across[d - 1])
            )
            outs[-1].start()
    for n in range(chunks):
        total = mine[n, pl.ds(pl.multiple_of(x * orows, 16), orows)]
        for d in range(1, nx):
            outs[n * (nx - 1) + d - 1].wait_recv()
            total = total + land[d - 1, n].astype(F32)
        out_ref[:, n * width : (n + 1) * width] = total.astype(BF16)
    for copy in gives + outs:
        copy.wait_send()
    for k in range(ny // 2):
        for m in range(2):
            for d in range(2):
                if k < hops(ny, d, m):
                    for copy in copies(d, m, k):
                        copy.wait_send()


def local(sp, tp, tokens, pre_gain, w_query, w_key, w_value, w_pool, lambdas, sub_gain, group_weight, pool_scale, w_out):
    nz, ny = grid_of(sp)
    nx = tp // 2
    rows, part = tokens.shape
    wrows = w_query.shape[0]
    head = w_value.shape[1]
    qd = w_query.shape[1]
    wide = 2 * qd + 2 * head
    cols = w_out.shape[1]
    scale = 1.0 / math.sqrt(qd // 2)
    dma = pltpu.SemaphoreType.DMA
    tok_full, w_full = call(
        functools.partial(gather_kernel, nz, ny, nx),
        (tokens, pre_gain.reshape(1, part), w_query, w_key, w_value, w_pool),
        (sds(tp, rows + 16, part), sds(nz, ny, 2, wrows // 2, wide)),
        [VMEM((rows + 16, part), BF16), VMEM((wrows, wide), BF16)]
        + [dma((2 * nx,)), dma((2 * nx,)), dma((ny,)), dma((ny,)), dma((nz,)), dma((nz,))]
        + ring_sems(nz, 2)
        + ring_sems(ny, 2),
        cid=0,
        name="gather",
    )
    qt, k, vt, pool = call(
        functools.partial(project_kernel, tp),
        (tok_full, w_full.reshape(sp * wrows, wide)),
        (sds(qd, rows), sds(rows, qd), sds(head, rows), sds(rows, head)),
        [VMEM((rows, tp * part), BF16), VMEM((rows, 128), F32)],
        name="project",
    )
    q_all, k_all, v_all, halo, wo_all = call(
        functools.partial(spread_kernel, nz, ny),
        (qt, k, vt, pool, w_out.T),
        (sds(ny, qd, rows), sds(nz, rows, qd), sds(nz, head, rows), sds(RIM, head), sds(nz, ny, cols, qd + head)),
        ring_sems(nz, 2) + ring_sems(ny, 2) + ring_sems(ny, 2) + [dma((nz,)), dma((nz,)), dma, dma],
        cid=1,
        name="spread",
    )
    acc, st = call(
        functools.partial(attend_kernel, nz, ny, scale),
        (q_all, k_all, v_all),
        (sds(ny, head, 2 * rows, dtype=F32), sds(ny, 8, 2 * rows, dtype=F32)),
        [VMEM((qd, 2 * rows), BF16), VMEM((8, 2 * rows), F32), VMEM((8, 2 * rows), F32)],
        name="attend",
    )
    half = ny // 2
    orows = rows // tp
    chunks, width = 4, sp * cols // 4
    (out,) = call(
        functools.partial(finish_kernel, ny, nx, scale),
        (
            acc,
            st,
            jnp.broadcast_to(lambdas.reshape(1, 1), (8, 128)),
            sub_gain.reshape(1, head),
            pool,
            halo,
            group_weight,
            pool_scale.reshape(1, head),
            wo_all.reshape(sp * cols, qd + head),
        ),
        (sds(orows, sp * cols),),
        [
            VMEM((head, rows), F32),
            VMEM((rows, 2 * head), BF16),
            VMEM((chunks, nx * orows, width), F32),
            VMEM((2, 2, half, head, rows), BF16),
            VMEM((2, 2, half, 8, rows), F32),
            VMEM((2, 2, half, head, rows), BF16),
            VMEM((2, 2, half, 8, rows), F32),
            VMEM((chunks, nx * orows, width), BF16),
            VMEM((chunks, nx * orows, width), BF16),
            VMEM((chunks, nx * orows, width), BF16),
            VMEM((max(nx - 1, 1), chunks, orows, width), BF16),
        ]
        + [dma((2, 2, half))] * 4
        + [dma((chunks,))] * 2
        + [dma((nx, chunks))] * 2,
        cid=2,
        name="finish",
    )
    return out


def solution(mesh):
    placed = (
        P("sp", "tp"),
        P("tp"),
        P("sp", "tp"),
        P("sp", "tp"),
        P("sp", "tp"),
        P("sp", "tp"),
        P("tp"),
        P(),
        P("tp", None, None),
        P("tp"),
        P("tp", "sp"),
    )
    body = functools.partial(local, mesh.shape["sp"], mesh.shape["tp"])
    return jax.shard_map(body, mesh=mesh, in_specs=placed, out_specs=P(("sp", "tp"), None), check_vma=False)
```

```python
import functools
import math

import jax
import jax.numpy as jnp
from jax import lax
from jax.experimental import pallas as pl
from jax.experimental.pallas import tpu as pltpu
from jax.sharding import PartitionSpec as P

MESH = pl.DeviceIdType.MESH
VMEM = pltpu.VMEM
EPSILON = 1e-06
NEG_LARGE = -1e30
F32, BF16 = jnp.float32, jnp.bfloat16
RIM = 16
DEPTH = 256
LEAD = 3


def grid_of(sp):
    ny = 2 ** ((sp.bit_length() - 1) // 2)
    return sp // ny, ny


def vspec(n):
    return [pl.BlockSpec(memory_space=VMEM)] * n


def sds(*shape, dtype=BF16):
    return jax.ShapeDtypeStruct(shape, dtype)


def call(kernel, ins, outs, scratch=(), cid=None, limit=40 << 20, name=None, flops=1 << 24):
    params = dict(vmem_limit_bytes=limit)
    if cid is not None:
        params.update(collective_id=cid, has_side_effects=True)
    return pl.pallas_call(
        kernel,
        out_shape=tuple(outs),
        in_specs=vspec(len(ins)),
        out_specs=tuple(vspec(len(outs))),
        scratch_shapes=list(scratch),
        compiler_params=pltpu.CompilerParams(**params),
        cost_estimate=pl.CostEstimate(flops=flops, bytes_accessed=1 << 20, transcendentals=0),
        name=name,
    )(*ins)


def rcopy(src, dst, ssem, rsem, dev):
    return pltpu.make_async_remote_copy(
        src_ref=src, dst_ref=dst, send_sem=ssem, recv_sem=rsem, device_id=dev, device_id_type=MESH
    )


def greet(peers):
    barrier = pltpu.get_barrier_semaphore()
    for dev in peers:
        pl.semaphore_signal(barrier, inc=1, device_id=dev, device_id_type=MESH)
    pl.semaphore_wait(barrier, len(peers))


def hops(n, direction, sub):
    return n // 2 if (direction + sub) % 2 == 0 else (n - 1) // 2


class Ring:
    def __init__(self, n, me, dev, piece, subs, ssem, rsem):
        self.n, self.me, self.dev, self.piece, self.subs = n, me, dev, piece, subs
        self.ssem, self.rsem = ssem, rsem
        self.steps = n // 2

    def copy(self, d, sub, k):
        sign = 1 if d == 0 else -1
        block = (self.me - sign * k) % self.n
        ref = self.piece(block, sub)
        return rcopy(
            ref, ref, self.ssem.at[d, sub, k], self.rsem.at[d, sub, k], self.dev((self.me + sign) % self.n)
        )

    def step(self, k):
        for sub in range(self.subs):
            for d in range(2):
                if k > 0 and k - 1 < hops(self.n, d, sub):
                    self.copy(d, sub, k - 1).wait_recv()
                if k < hops(self.n, d, sub):
                    self.copy(d, sub, k).start()

    def finish(self):
        for k in range(self.steps):
            for sub in range(self.subs):
                for d in range(2):
                    if k < hops(self.n, d, sub):
                        self.copy(d, sub, k).wait_send()


def ring_sems(n, subs):
    return [pltpu.SemaphoreType.DMA((2, subs, n // 2)), pltpu.SemaphoreType.DMA((2, subs, n // 2))]


def gather_kernel(nz, ny, nx, tin_ref, gain_ref, wq_ref, wk_ref, wv_ref, wp_ref, tok_full, w_full, tok_ref, w_ref, ts, tr, ys, yr, zs, zr, as_, ar, bs, br):
    s, t = lax.axis_index("sp"), lax.axis_index("tp")
    z, y, x, c = s // ny, s % ny, t // 2, t % 2
    half = w_ref.shape[0] // 2
    rows = tin_ref.shape[0]
    tok_ref[0:rows] = tin_ref[...]
    tok_ref[rows:] = jnp.broadcast_to(gain_ref[...], (16, gain_ref.shape[1]))
    at = 0
    for ref in (wq_ref, wk_ref, wv_ref, wp_ref):
        w_ref[:, at : at + ref.shape[1]] = ref[...]
        at += ref.shape[1]
    partner = (s, x * 2 + 1 - c)
    across = [(s, ((x + d) % nx) * 2 + c) for d in range(1, nx)]
    along_y = [(z * ny + (y + d) % ny, t) for d in range(1, ny)]
    along_z = [(((z + d) % nz) * ny + y, t) for d in range(1, nz)]
    greet([partner] + across + along_y + along_z)

    ysends = [
        rcopy(w_ref.at[0:half], w_full.at[z, y, 0], ys.at[d], yr.at[d], along_y[d]) for d in range(ny - 1)
    ]
    zsends = [
        rcopy(w_ref.at[half:], w_full.at[z, y, 1], zs.at[d], zr.at[d], along_z[d]) for d in range(nz - 1)
    ]
    tsends = [rcopy(tok_ref, tok_full.at[t], ts.at[d], tr.at[d], across[d]) for d in range(nx - 1)]
    tsends.append(rcopy(tok_ref, tok_full.at[t], ts.at[nx - 1], tr.at[nx - 1], partner))
    for copy in ysends + zsends + tsends:
        copy.start()
    w_full[z, y, 0] = w_ref[0:half]
    w_full[z, y, 1] = w_ref[half:]
    tok_full[t] = tok_ref[...]

    def piece_a(block, sub):
        return w_full.at[block, sub * (ny // 2) : (sub + 1) * (ny // 2), 0]

    def piece_b(block, sub):
        return w_full.at[sub * (nz // 2) : (sub + 1) * (nz // 2), block, 1]

    ring_a = Ring(nz, z, lambda i: (i * ny + y, t), piece_a, 2, as_, ar)
    ring_b = Ring(ny, y, lambda i: (z * ny + i, t), piece_b, 2, bs, br)
    for copy in ysends:
        copy.wait_recv()
    ring_a.step(0)
    for copy in zsends:
        copy.wait_recv()
    ring_b.step(0)
    relays = []
    for k in range(1, max(ring_a.steps, ring_b.steps) + 1):
        if k <= ring_a.steps:
            ring_a.step(k)
        if k <= ring_b.steps:
            ring_b.step(k)
        if k == 1:
            for d in range(nx - 1):
                tsends[d].wait_recv()
                source = ((x - 1 - d) % nx) * 2 + c
                relays.append(
                    rcopy(tok_full.at[source], tok_full.at[source], ts.at[nx + d], tr.at[nx + d], partner)
                )
                relays[-1].start()
    tsends[-1].wait_recv()
    for copy in relays:
        copy.wait_recv()
    for copy in ysends + zsends + tsends + relays:
        copy.wait_send()
    ring_a.finish()
    ring_b.finish()


def project_kernel(tp, tok_ref, w_ref, qt_ref, k_ref, vt_ref, pool_ref, scaled, sq):
    rows, part = qt_ref.shape[1], tok_ref.shape[2]
    sq[...] = jnp.zeros_like(sq)
    for t in range(tp):
        x = tok_ref[t, 0:rows].astype(F32)
        gain = tok_ref[t, rows : rows + 1].astype(F32)
        squares = x * x
        for i in range(part // 128):
            sq[...] += squares[:, i * 128 : (i + 1) * 128]
        scaled[:, t * part : (t + 1) * part] = (x * gain).astype(BF16)
    inverse = lax.rsqrt(jnp.sum(sq[...], axis=1, keepdims=True) / (tp * part) + EPSILON)

    def project(at):
        out = jnp.dot(scaled[...], w_ref[:, at * 128 : at * 128 + 256], preferred_element_type=F32) * inverse
        return out[:, 0:128].astype(BF16), out[:, 128:256].astype(BF16)

    q, k = project(0)
    qt_ref[...] = jnp.transpose(q.astype(F32)).astype(BF16)
    k_ref[...] = k
    v, p = project(2)
    vt_ref[...] = jnp.transpose(v.astype(F32)).astype(BF16)
    pool_ref[...] = p


def attend_kernel(
    nz, ny, scale, q_ref, k_ref, v_ref, p_ref, wo_ref, q_all, k_all, v_all, halo, wo_all, acc_ref, st_ref,
    qz_ref, sum_ref, zs, zr, ys, yr, os, or_, ws, wr, hs, hr,
):
    s, t = lax.axis_index("sp"), lax.axis_index("tp")
    z, y = s // ny, s % ny
    sp = nz * ny
    dev_z = lambda i: (i * ny + y, t)
    dev_y = lambda i: (z * ny + i, t)
    rows = p_ref.shape[0]
    nxt, prv = ((s + 1) % sp, t), ((s + sp - 1) % sp, t)
    along_z = [dev_z((z + d) % nz) for d in range(1, nz)]
    greet(along_z + [dev_y((y + 1) % ny), dev_y((y + ny - 1) % ny), nxt, prv])
    q_all[y] = q_ref[...]
    k_all[z] = k_ref[...]
    v_all[z] = v_ref[...]
    wo_all[z, y] = wo_ref[...]
    dim = q_ref.shape[0]
    half = dim // 2
    ring_y = Ring(ny, y, dev_y, lambda b, i: q_all.at[b, i * half : (i + 1) * half], 2, ys, yr)
    ring_z = Ring(nz, z, dev_z, lambda b, i: (k_all if i == 0 else v_all).at[b], 2, zs, zr)
    ring_o = Ring(ny, y, dev_y, lambda b, i: wo_all.at[i * (nz // 2) : (i + 1) * (nz // 2), b], 2, os, or_)
    ring_y.step(0)
    ring_z.step(0)
    wcopies = [rcopy(wo_ref, wo_all.at[z, y], ws.at[d], wr.at[d], along_z[d]) for d in range(nz - 1)]
    hcopy = rcopy(p_ref.at[rows - RIM :], halo, hs, hr, nxt)
    for copy in wcopies + [hcopy]:
        copy.start()

    lanes = 2 * rows
    width = min(256, rows)
    vd = v_all.shape[1]
    factor = scale / math.log(2.0)

    def positions(yq, at, wide):
        lane = lax.broadcasted_iota(jnp.int32, (1, wide), 1) + at
        return jnp.where(lane >= rows, lane - rows, lane) + (z * ny + yq) * rows

    def begin(yq):
        qt = q_all[yq]
        low = lax.broadcasted_iota(jnp.int32, qt.shape, 0) < half
        zero = jnp.zeros_like(qt)
        qz_ref[yq, :, 0:rows] = jnp.where(low, qt, zero)
        qz_ref[yq, :, rows:] = jnp.where(low, zero, qt)
        acc_ref[yq] = jnp.zeros((vd, lanes), F32)
        sum_ref[yq] = jnp.zeros((8, lanes), F32)
        few = min(128, rows)
        source = jnp.where(yq >= y, z, jnp.maximum(z - 1, 0))
        sc = jnp.dot(k_all[source, 0:few], qz_ref[yq], preferred_element_type=F32)
        kpos = (source * ny + y) * rows + lax.broadcasted_iota(jnp.int32, (few, 1), 0)
        bar = jnp.max(jnp.where(kpos <= positions(yq, 0, lanes), sc, NEG_LARGE), axis=0, keepdims=True)
        st_ref[yq, 0:1] = bar
        st_ref[yq, 1:2] = bar * factor

    def tiles(yq, blocks, mask=None):
        keys = jnp.concatenate([k_all[b] for b in blocks], axis=0)
        vals = jnp.concatenate([v_all[b] for b in blocks], axis=1)
        depth = rows if len(blocks) == 1 else min(DEPTH, rows)
        work = [(at, low) for at in range(0, lanes, width) for low in range(0, keys.shape[0], depth)]

        def scores(item):
            at, low = item
            return jnp.dot(keys[low : low + depth], qz_ref[yq, :, at : at + width], preferred_element_type=F32)

        ahead = [scores(item) for item in work[:LEAD]]
        total, gain = None, None
        for i, (at, low) in enumerate(work):
            sc = ahead.pop(0)
            if i + LEAD < len(work):
                ahead.append(scores(work[i + LEAD]))
            cols = slice(at, at + width)
            expo = jnp.exp2(sc * factor - st_ref[yq, 1:2, cols])
            if mask is not None:
                expo = jnp.where(mask(at)[low : low + depth], expo, 0.0)
            part = jnp.sum(expo.reshape(depth // 8, 8, width), axis=0)
            total = part if low == 0 else total + part
            term = jnp.dot(vals[:, low : low + depth], expo.astype(BF16), preferred_element_type=F32)
            gain = term if low == 0 else gain + term
            if low + depth == keys.shape[0]:
                sum_ref[yq, :, cols] += total
                acc_ref[yq, :, cols] += gain

    def visits(k, first, last):
        def visit(i, carry):
            yq = lax.rem(y + i + (ny - k), ny)
            new = jnp.logical_or(i == 0, i == 2 * k)

            @pl.when(new)
            def _():
                begin(yq)

                @pl.when(yq > y)
                def _():
                    tiles(yq, [z])

            def at_distance(j, carry):
                below = z >= j
                above = jnp.logical_and(z + j >= nz, 2 * j < nz)

                @pl.when(jnp.logical_and(below, above))
                def _():
                    tiles(yq, [lax.rem(z + nz - j, nz), lax.rem(z + j, nz)])

                @pl.when(jnp.logical_xor(below, above))
                def _():
                    tiles(yq, [lax.rem(jnp.where(below, z + nz - j, z + j), nz)])

                return carry

            return lax.fori_loop(jnp.where(new, 1, k), k + 1, at_distance, carry)

        lax.fori_loop(first, last, visit, 0)

    begin(y)
    kpos = (z * ny + y) * rows + lax.broadcasted_iota(jnp.int32, (rows, 1), 0)
    tiles(y, [z], lambda at: kpos <= positions(y, at, width))
    steps = max(ring_y.steps, ring_z.steps)

    def advance(k):
        ring_z.step(k)
        ring_y.step(k)
        if k == 1:
            for copy in wcopies:
                copy.wait_recv()
        ring_o.step(k - 1)

    advance(1)
    for k in range(1, steps + 1):
        last = 2 * k if 2 * k == ny else 2 * k + 1
        if k == 3 and steps > 3:
            visits(k, 0, k)
            advance(k + 1)
            visits(k, k, last)
        else:
            visits(k, 0, last)
            if k < steps:
                advance(k + 1)
    ring_o.step(steps)
    for b in range(ny):
        st_ref[b, 1:2] = jnp.sum(sum_ref[b], axis=0, keepdims=True)
    hcopy.wait_recv()
    for copy in wcopies + [hcopy]:
        copy.wait_send()
    ring_z.finish()
    ring_y.finish()
    ring_o.finish()


def repair_kernel(ny, scale, q_all, k_all, v_all, acc_in, st_in, acc_ref, st_ref, qz_ref):
    s = lax.axis_index("sp")
    z, y = s // ny, s % ny
    rows = q_all.shape[2]
    half = q_all.shape[1] // 2
    lanes = 2 * rows
    factor = scale / math.log(2.0)
    calm = jnp.max(st_in[:, 1:2]) < 2.0**80

    @pl.when(calm)
    def _():
        acc_ref[...] = acc_in[...]
        st_ref[:, 0:2] = st_in[:, 0:2]

    @pl.when(jnp.logical_not(calm))
    def _():
        def slow(yq, carry):
            qt = q_all[yq]
            low = lax.broadcasted_iota(jnp.int32, qt.shape, 0) < half
            zero = jnp.zeros_like(qt)
            qz_ref[:, 0:rows] = jnp.where(low, qt, zero)
            qz_ref[:, rows:] = jnp.where(low, zero, qt)
            acc_ref[yq] = jnp.zeros((acc_ref.shape[1], lanes), F32)
            st_ref[yq, 0:1] = jnp.full((1, lanes), NEG_LARGE, F32)
            st_ref[yq, 1:2] = jnp.zeros((1, lanes), F32)

            def block(b, carry):
                kpos = (b * ny + y) * rows + lax.broadcasted_iota(jnp.int32, (rows, 1), 0)

                def group(g, carry):
                    at = pl.multiple_of(g * 128, 128)
                    cols = pl.ds(at, 128)
                    lane = lax.broadcasted_iota(jnp.int32, (1, 128), 1) + at
                    qpos = jnp.where(lane >= rows, lane - rows, lane) + (z * ny + yq) * rows
                    allowed = kpos <= qpos
                    sc = jnp.dot(k_all[b], qz_ref[:, cols], preferred_element_type=F32)
                    sc = jnp.where(allowed, sc, NEG_LARGE)
                    old = st_ref[yq, 0:1, cols]
                    new = jnp.maximum(old, jnp.max(sc, axis=0, keepdims=True))
                    expo = jnp.where(allowed, jnp.exp2((sc - new) * factor), 0.0)
                    shrink = jnp.exp2((old - new) * factor)
                    st_ref[yq, 0:1, cols] = new
                    st_ref[yq, 1:2, cols] = st_ref[yq, 1:2, cols] * shrink + jnp.sum(expo, axis=0, keepdims=True)
                    acc_ref[yq, :, cols] = acc_ref[yq, :, cols] * shrink + jnp.dot(
                        v_all[b], expo.astype(BF16), preferred_element_type=F32
                    )
                    return carry

                return lax.fori_loop(0, lanes // 128, group, carry)

            return lax.fori_loop(0, z + 1, block, carry)

        lax.fori_loop(0, ny, slow, 0)


def finish_kernel(
    ny, nx, scale, acc_ref, st_ref, lam_ref, gain_ref, p_ref, halo, gw_ref, ps_ref, wo_ref, out_ref,
    mix, branch, mine, wbuf, sbuf, wland, sland, give, take, send, land, ws, wr, ss, sr, gs, gr, os, or_,
):
    s, t = lax.axis_index("sp"), lax.axis_index("tp")
    z, y, x, c = s // ny, s % ny, t // 2, t % 2
    rows, head = p_ref.shape
    orows = out_ref.shape[0]
    chunks, _, width = mine.shape
    factor = scale / math.log(2.0)
    dev = lambda i: (z * ny + i % ny, t)
    partner = (s, x * 2 + 1 - c)
    across = [(s, ((x + d) % nx) * 2 + c) for d in range(1, nx)]
    greet([dev(y + 1), dev(y + ny - 1), partner] + across)

    def pooled():
        here = p_ref[...].astype(F32)
        rim = jnp.where(s > 0, halo[...].astype(F32), 0.0)
        total = jnp.concatenate([rim, here], axis=0)
        slot = t % 4
        for i in range(4):
            more = total + pltpu.roll(total, 1 << i, 0)
            total = jnp.where(i <= slot, more, total)
        span = jnp.where(slot == 0, 2, jnp.where(slot == 1, 4, jnp.where(slot == 2, 8, 16)))
        pos = s * rows + lax.broadcasted_iota(jnp.int32, (rows, 1), 0)
        count = jnp.minimum(pos + 1, span).astype(F32)
        differ = (total[RIM:] / count - here).astype(BF16)
        return (jnp.dot(differ, gw_ref[0], preferred_element_type=F32) * ps_ref[...]).astype(BF16)

    def own(block, m):
        cols = slice(m * rows, (m + 1) * rows)
        return acc_ref[block, :, cols], st_ref[block, 0:1, cols], st_ref[block, 1:2, cols]

    def joined(a, b):
        top = jnp.maximum(a[1], b[1])
        fa, fb = jnp.exp2((a[1] - top) * factor), jnp.exp2((b[1] - top) * factor)
        return a[0] * fa + b[0] * fb, top, a[2] * fa + b[2] * fb

    def landed(d, m, k):
        return wland[d, m, k].astype(F32), sland[d, m, k, 0:1], sland[d, m, k, 1:2]

    def copies(d, m, k):
        to = dev(y + (1 if d == 0 else ny - 1))
        return [
            rcopy(wbuf.at[d, m, k], wland.at[d, m, k], ws.at[d, m, k], wr.at[d, m, k], to),
            rcopy(sbuf.at[d, m, k], sland.at[d, m, k], ss.at[d, m, k], sr.at[d, m, k], to),
        ]

    for k in range(ny // 2):
        for m in range(2):
            for d in range(2):
                n = hops(ny, d, m)
                if k >= n:
                    continue
                sign = 1 if d == 0 else -1
                block = (y + sign * (n - k)) % ny
                state = own(block, m)
                if k > 0:
                    for copy in copies(d, m, k - 1):
                        copy.wait_recv()
                    state = joined(state, landed(d, m, k - 1))
                wbuf[d, m, k] = state[0].astype(BF16)
                sbuf[d, m, k, 0:1] = state[1]
                sbuf[d, m, k, 1:2] = state[2]
                for copy in copies(d, m, k):
                    copy.start()
        if k == 0:
            branch[:, head:] = pooled()
    for m in range(2):
        state = own(y, m)
        for d in range(2):
            n = hops(ny, d, m)
            if n > 0:
                for copy in copies(d, m, n - 1):
                    copy.wait_recv()
                state = joined(state, landed(d, m, n - 1))
        if m == 0:
            mix[...] = state[0] / state[2]
        else:
            mix[...] = mix[...] - lam_ref[0:1, 0:1] * state[0] / state[2]
    mixed = mix[...]
    mean = jnp.mean(mixed * mixed, axis=0, keepdims=True)
    normed = jnp.transpose(mixed * lax.rsqrt(mean + EPSILON)) * gain_ref[...]
    branch[:, 0:head] = normed.astype(BF16)

    def rows_of(core):
        starts = [pl.multiple_of((2 * i + core) * orows, 16) for i in range(nx)]
        return jnp.concatenate([branch[pl.ds(at, orows)] for at in starts], axis=0)

    def product(lhs, n):
        return lax.dot_general(
            lhs, wo_ref[n * width : (n + 1) * width], (((1,), (1,)), ((), ())), preferred_element_type=F32
        )

    lhs = rows_of(1 - c)
    gives = [rcopy(give.at[n], take.at[n], gs.at[n], gr.at[n], partner) for n in range(chunks)]
    for n in range(chunks):
        give[n] = product(lhs, n).astype(BF16)
        gives[n].start()
    lhs = rows_of(c)
    for n in range(chunks):
        mine[n] = product(lhs, n)
    outs = []
    for n in range(chunks):
        gives[n].wait_recv()
        both = mine[n] + take[n].astype(F32)
        mine[n] = both
        send[n] = both.astype(BF16)
        for d in range(1, nx):
            at = pl.multiple_of(((x + d) % nx) * orows, 16)
            outs.append(
                rcopy(send.at[n, pl.ds(at, orows)], land.at[d - 1, n], os.at[d - 1, n], or_.at[d - 1, n], across[d - 1])
            )
            outs[-1].start()
    for n in range(chunks):
        total = mine[n, pl.ds(pl.multiple_of(x * orows, 16), orows)]
        for d in range(1, nx):
            outs[n * (nx - 1) + d - 1].wait_recv()
            total = total + land[d - 1, n].astype(F32)
        out_ref[:, n * width : (n + 1) * width] = total.astype(BF16)
    for copy in gives + outs:
        copy.wait_send()
    for k in range(ny // 2):
        for m in range(2):
            for d in range(2):
                if k < hops(ny, d, m):
                    for copy in copies(d, m, k):
                        copy.wait_send()


def local(sp, tp, tokens, pre_gain, w_query, w_key, w_value, w_pool, lambdas, sub_gain, group_weight, pool_scale, w_out):
    nz, ny = grid_of(sp)
    nx = tp // 2
    rows, part = tokens.shape
    wrows = w_query.shape[0]
    head = w_value.shape[1]
    qd = w_query.shape[1]
    wide = 2 * qd + 2 * head
    cols = w_out.shape[1]
    scale = 1.0 / math.sqrt(qd // 2)
    dma = pltpu.SemaphoreType.DMA
    tok_full, w_full = call(
        functools.partial(gather_kernel, nz, ny, nx),
        (tokens, pre_gain.reshape(1, part), w_query, w_key, w_value, w_pool),
        (sds(tp, rows + 16, part), sds(nz, ny, 2, wrows // 2, wide)),
        [VMEM((rows + 16, part), BF16), VMEM((wrows, wide), BF16)]
        + [dma((2 * nx,)), dma((2 * nx,)), dma((ny,)), dma((ny,)), dma((nz,)), dma((nz,))]
        + ring_sems(nz, 2)
        + ring_sems(ny, 2),
        cid=0,
        name="gather",
    )
    qt, k, vt, pool = call(
        functools.partial(project_kernel, tp),
        (tok_full, w_full.reshape(sp * wrows, wide)),
        (sds(qd, rows), sds(rows, qd), sds(head, rows), sds(rows, head)),
        [VMEM((rows, tp * part), BF16), VMEM((rows, 128), F32)],
        name="project",
    )
    totals = (sds(ny, head, 2 * rows, dtype=F32), sds(ny, 8, 2 * rows, dtype=F32))
    q_all, k_all, v_all, halo, wo_all, acc, st = call(
        functools.partial(attend_kernel, nz, ny, scale),
        (qt, k, vt, pool, w_out.T),
        (sds(ny, qd, rows), sds(nz, rows, qd), sds(nz, head, rows), sds(RIM, head), sds(nz, ny, cols, qd + head))
        + totals,
        [VMEM((ny, qd, 2 * rows), BF16), VMEM((ny, 8, 2 * rows), F32)]
        + ring_sems(nz, 2) + ring_sems(ny, 2) + ring_sems(ny, 2) + [dma((nz,)), dma((nz,)), dma, dma],
        cid=1,
        name="attend",
    )
    acc, st = call(
        functools.partial(repair_kernel, ny, scale),
        (q_all, k_all, v_all, acc, st),
        totals,
        [VMEM((qd, 2 * rows), BF16)],
        name="repair",
    )
    half = ny // 2
    orows = rows // tp
    chunks, width = 4, sp * cols // 4
    (out,) = call(
        functools.partial(finish_kernel, ny, nx, scale),
        (
            acc,
            st,
            jnp.broadcast_to(lambdas.reshape(1, 1), (8, 128)),
            sub_gain.reshape(1, head),
            pool,
            halo,
            group_weight,
            pool_scale.reshape(1, head),
            wo_all.reshape(sp * cols, qd + head),
        ),
        (sds(orows, sp * cols),),
        [
            VMEM((head, rows), F32),
            VMEM((rows, 2 * head), BF16),
            VMEM((chunks, nx * orows, width), F32),
            VMEM((2, 2, half, head, rows), BF16),
            VMEM((2, 2, half, 8, rows), F32),
            VMEM((2, 2, half, head, rows), BF16),
            VMEM((2, 2, half, 8, rows), F32),
            VMEM((chunks, nx * orows, width), BF16),
            VMEM((chunks, nx * orows, width), BF16),
            VMEM((chunks, nx * orows, width), BF16),
            VMEM((max(nx - 1, 1), chunks, orows, width), BF16),
        ]
        + [dma((2, 2, half))] * 4
        + [dma((chunks,))] * 2
        + [dma((nx, chunks))] * 2,
        cid=2,
        name="finish",
    )
    return out


def solution(mesh):
    placed = (
        P("sp", "tp"),
        P("tp"),
        P("sp", "tp"),
        P("sp", "tp"),
        P("sp", "tp"),
        P("sp", "tp"),
        P("tp"),
        P(),
        P("tp", None, None),
        P("tp"),
        P("tp", "sp"),
    )
    body = functools.partial(local, mesh.shape["sp"], mesh.shape["tp"])
    return jax.shard_map(body, mesh=mesh, in_specs=placed, out_specs=P(("sp", "tp"), None), check_vma=False)
```

```python
import functools
import math

import jax
import jax.numpy as jnp
from jax import lax
from jax.experimental import pallas as pl
from jax.experimental.pallas import tpu as pltpu
from jax.sharding import PartitionSpec as P

MESH = pl.DeviceIdType.MESH
VMEM = pltpu.VMEM
EPSILON = 1e-06
NEG_LARGE = -1e30
F32, BF16 = jnp.float32, jnp.bfloat16
RIM = 16
DEPTH = 256
LEAD = 3
PARTS, EARLY = 8, 6


def grid_of(sp):
    ny = 2 ** ((sp.bit_length() - 1) // 2)
    return sp // ny, ny


def vspec(n):
    return [pl.BlockSpec(memory_space=VMEM)] * n


def sds(*shape, dtype=BF16):
    return jax.ShapeDtypeStruct(shape, dtype)


def call(kernel, ins, outs, scratch=(), cid=None, limit=40 << 20, name=None, flops=1 << 24, space=VMEM):
    params = dict(vmem_limit_bytes=limit)
    if cid is not None:
        params.update(collective_id=cid, has_side_effects=True)
    return pl.pallas_call(
        kernel,
        out_shape=tuple(outs),
        in_specs=[pl.BlockSpec(memory_space=space)] * len(ins),
        out_specs=tuple(vspec(len(outs))),
        scratch_shapes=list(scratch),
        compiler_params=pltpu.CompilerParams(**params),
        cost_estimate=pl.CostEstimate(flops=flops, bytes_accessed=1 << 20, transcendentals=0),
        name=name,
    )(*ins)


def rcopy(src, dst, ssem, rsem, dev):
    return pltpu.make_async_remote_copy(
        src_ref=src, dst_ref=dst, send_sem=ssem, recv_sem=rsem, device_id=dev, device_id_type=MESH
    )


def greet(peers):
    barrier = pltpu.get_barrier_semaphore()
    for dev in peers:
        pl.semaphore_signal(barrier, inc=1, device_id=dev, device_id_type=MESH)
    pl.semaphore_wait(barrier, len(peers))


def hops(n, direction, sub):
    return n // 2 if (direction + sub) % 2 == 0 else (n - 1) // 2


class Ring:
    def __init__(self, n, me, dev, piece, subs, ssem, rsem):
        self.n, self.me, self.dev, self.piece, self.subs = n, me, dev, piece, subs
        self.ssem, self.rsem = ssem, rsem
        self.steps = n // 2

    def copy(self, d, sub, k):
        sign = 1 if d == 0 else -1
        block = (self.me - sign * k) % self.n
        ref = self.piece(block, sub)
        return rcopy(
            ref, ref, self.ssem.at[d, sub, k], self.rsem.at[d, sub, k], self.dev((self.me + sign) % self.n)
        )

    def step(self, k, subs=None, landed=None):
        for sub in subs if subs is not None else range(self.subs):
            for d in range(2):
                if k > 0 and k - 1 < hops(self.n, d, sub):
                    self.copy(d, sub, k - 1).wait_recv()
                    if landed is not None:
                        landed((self.me + (k if d else -k)) % self.n, sub)
                if k < hops(self.n, d, sub):
                    self.copy(d, sub, k).start()

    def finish(self):
        for k in range(self.steps):
            for sub in range(self.subs):
                for d in range(2):
                    if k < hops(self.n, d, sub):
                        self.copy(d, sub, k).wait_send()


def ring_sems(n, subs):
    return [pltpu.SemaphoreType.DMA((2, subs, max(n // 2, 1))), pltpu.SemaphoreType.DMA((2, subs, max(n // 2, 1)))]


class Shared:
    def __init__(self, nx, own, buf, subs, size, rs, rr, ps, pr):
        s, t = lax.axis_index("sp"), lax.axis_index("tp")
        x, c = t // 2, t % 2
        self.nx, self.x, self.c, self.t = nx, x, c, t
        self.buf, self.ps, self.pr, self.own = buf, ps, pr, own
        self.partner = (s, x * 2 + 1 - c)
        self.peers = [(s, ((x + d) % nx) * 2 + c) for d in ((1, nx - 1) if nx > 1 else ())] + [self.partner]
        self.piece = lambda b, i: buf.at[2 * b + c, i * size : (i + 1) * size]
        self.ring = Ring(nx, x, lambda i: (s, 2 * i + c), self.piece, subs, rs, rr)
        self.subs = subs
        self.relays = []

    def relay(self, block, sub):
        ref = self.piece(block, sub)
        at = len(self.relays)
        copy = rcopy(ref, ref, self.ps.at[at], self.pr.at[at], self.partner)
        copy.start()
        self.relays.append(copy)

    def start(self):
        self.buf[self.t] = self.own[...]
        self.ring.step(0)
        self.direct = rcopy(
            self.own, self.buf.at[self.t], self.ps.at[self.subs * self.nx], self.pr.at[self.subs * self.nx], self.partner
        )
        self.direct.start()

    def step(self, k, subs):
        if k <= self.ring.steps:
            self.ring.step(k, subs, self.relay)

    def finish(self):
        for copy in self.relays + [self.direct]:
            copy.wait_recv()
        for copy in self.relays + [self.direct]:
            copy.wait_send()
        self.ring.finish()


def shared_sems(nx, subs):
    dma = pltpu.SemaphoreType.DMA
    return ring_sems(nx, subs) + [dma((subs * nx + 1,)), dma((subs * nx + 1,))]


def gather_kernel(nz, ny, nx, tin_ref, gain_ref, wq_ref, wk_ref, wv_ref, wp_ref, wo_ref, tok_full, w_full, tok_ref, w_ref, gain, ins, ts, tr, ys, yr, zs, zr, as_, ar, bs, br):
    s, t = lax.axis_index("sp"), lax.axis_index("tp")
    z, y, x, c = s // ny, s % ny, t // 2, t % 2
    half = w_ref.shape[0] // 2
    rows = tin_ref.shape[0]
    loads = [pltpu.make_async_copy(tin_ref, tok_ref.at[0:rows], ins.at[0]), pltpu.make_async_copy(gain_ref, gain, ins.at[1])]
    at = 0
    for i, ref in enumerate((wq_ref, wk_ref, wv_ref, wp_ref, wo_ref)):
        loads.append(pltpu.make_async_copy(ref, w_ref.at[:, at : at + ref.shape[1]], ins.at[2 + i]))
        at += ref.shape[1]
    for load in loads:
        load.start()
    loads[1].wait()
    tok_ref[rows:] = jnp.broadcast_to(gain[...], (16, gain.shape[1]))
    partner = (s, x * 2 + 1 - c)
    across = [(s, ((x + d) % nx) * 2 + c) for d in range(1, nx)]
    along_y = [(z * ny + (y + d) % ny, t) for d in range(1, ny)]
    along_z = [(((z + d) % nz) * ny + y, t) for d in range(1, nz)]
    greet([partner] + across + along_y + along_z)
    for i, load in enumerate(loads):
        if i != 1:
            load.wait()

    ysends = [
        rcopy(w_ref.at[0:half], w_full.at[z, y, 0], ys.at[d], yr.at[d], along_y[d]) for d in range(ny - 1)
    ]
    zsends = [
        rcopy(w_ref.at[half:], w_full.at[z, y, 1], zs.at[d], zr.at[d], along_z[d]) for d in range(nz - 1)
    ]
    tsends = [rcopy(tok_ref, tok_full.at[t], ts.at[d], tr.at[d], across[d]) for d in range(nx - 1)]
    tsends.append(rcopy(tok_ref, tok_full.at[t], ts.at[nx - 1], tr.at[nx - 1], partner))
    for copy in ysends + zsends + tsends:
        copy.start()
    w_full[z, y, 0] = w_ref[0:half]
    w_full[z, y, 1] = w_ref[half:]
    tok_full[t] = tok_ref[...]

    def piece_a(block, sub):
        return w_full.at[block, sub * (ny // 2) : (sub + 1) * (ny // 2), 0]

    def piece_b(block, sub):
        return w_full.at[sub * (nz // 2) : (sub + 1) * (nz // 2), block, 1]

    ring_a = Ring(nz, z, lambda i: (i * ny + y, t), piece_a, 2, as_, ar)
    ring_b = Ring(ny, y, lambda i: (z * ny + i, t), piece_b, 2, bs, br)
    for copy in ysends:
        copy.wait_recv()
    ring_a.step(0)
    for copy in zsends:
        copy.wait_recv()
    ring_b.step(0)
    relays = []
    for k in range(1, max(ring_a.steps, ring_b.steps) + 1):
        if k <= ring_a.steps:
            ring_a.step(k)
        if k <= ring_b.steps:
            ring_b.step(k)
        if k == 1:
            for d in range(nx - 1):
                tsends[d].wait_recv()
                source = ((x - 1 - d) % nx) * 2 + c
                relays.append(
                    rcopy(tok_full.at[source], tok_full.at[source], ts.at[nx + d], tr.at[nx + d], partner)
                )
                relays[-1].start()
    tsends[-1].wait_recv()
    for copy in relays:
        copy.wait_recv()
    for copy in ysends + zsends + tsends + relays:
        copy.wait_send()
    ring_a.finish()
    ring_b.finish()


def project_kernel(tp, tok_ref, w_ref, qt_ref, k_ref, vt_ref, pool_ref, early, late, scaled, sq):
    rows, part = qt_ref.shape[1], tok_ref.shape[2]
    early[...] = w_ref[0 : early.shape[0], 512:]
    late[...] = w_ref[early.shape[0] :, 512:]
    sq[...] = jnp.zeros_like(sq)
    for t in range(tp):
        x = tok_ref[t, 0:rows].astype(F32)
        gain = tok_ref[t, rows : rows + 1].astype(F32)
        squares = x * x
        for i in range(part // 128):
            sq[...] += squares[:, i * 128 : (i + 1) * 128]
        scaled[:, t * part : (t + 1) * part] = (x * gain).astype(BF16)
    inverse = lax.rsqrt(jnp.sum(sq[...], axis=1, keepdims=True) / (tp * part) + EPSILON)

    def project(at):
        out = jnp.dot(scaled[...], w_ref[:, at * 128 : at * 128 + 256], preferred_element_type=F32) * inverse
        return out[:, 0:128].astype(BF16), out[:, 128:256].astype(BF16)

    q, k = project(0)
    qt_ref[...] = jnp.transpose(q.astype(F32)).astype(BF16)
    k_ref[...] = k
    v, p = project(2)
    vt_ref[...] = jnp.transpose(v.astype(F32)).astype(BF16)
    pool_ref[...] = p


def attend_kernel(
    nz, ny, nx, scale, q_ref, k_ref, v_ref, p_ref, wo_ref, q_all, k_all, v_all, halo, wo_all, acc_ref, st_ref,
    qz_ref, sum_ref, zs, zr, ys, yr, xs, xr, ps, pr, hs, hr,
):
    s, t = lax.axis_index("sp"), lax.axis_index("tp")
    z, y = s // ny, s % ny
    sp = nz * ny
    dev_z = lambda i: (i * ny + y, t)
    dev_y = lambda i: (z * ny + i, t)
    rows = p_ref.shape[0]
    nxt, prv = ((s + 1) % sp, t), ((s + sp - 1) % sp, t)
    shared = Shared(nx, wo_ref, wo_all, EARLY, wo_ref.shape[0] // EARLY, xs, xr, ps, pr)
    near = [dev_z((z + 1) % nz), dev_z((z + nz - 1) % nz), dev_y((y + 1) % ny), dev_y((y + ny - 1) % ny)]
    greet(near + [nxt, prv] + shared.peers)
    q_all[y] = q_ref[...]
    k_all[z] = k_ref[...]
    v_all[z] = v_ref[...]
    half = q_ref.shape[0] // 2
    ring_y = Ring(ny, y, dev_y, lambda b, i: q_all.at[b, i * half : (i + 1) * half], 2, ys, yr)
    ring_z = Ring(nz, z, dev_z, lambda b, i: (k_all if i == 0 else v_all).at[b], 2, zs, zr)
    ring_y.step(0)
    ring_z.step(0)
    shared.start()
    hcopy = rcopy(p_ref.at[rows - RIM :], halo, hs, hr, nxt)
    hcopy.start()

    lanes = 2 * rows
    width = min(256, rows)
    vd = v_all.shape[1]
    factor = scale / math.log(2.0)

    def positions(yq, at, wide):
        lane = lax.broadcasted_iota(jnp.int32, (1, wide), 1) + at
        return jnp.where(lane >= rows, lane - rows, lane) + (z * ny + yq) * rows

    def begin(yq):
        qt = q_all[yq]
        low = lax.broadcasted_iota(jnp.int32, qt.shape, 0) < half
        zero = jnp.zeros_like(qt)
        qz_ref[yq, :, 0:rows] = jnp.where(low, qt, zero)
        qz_ref[yq, :, rows:] = jnp.where(low, zero, qt)
        acc_ref[yq] = jnp.zeros((vd, lanes), F32)
        sum_ref[yq] = jnp.zeros((8, lanes), F32)
        few = min(128, rows)
        source = jnp.where(yq >= y, z, jnp.maximum(z - 1, 0))
        sc = jnp.dot(k_all[source, 0:few], qz_ref[yq], preferred_element_type=F32)
        kpos = (source * ny + y) * rows + lax.broadcasted_iota(jnp.int32, (few, 1), 0)
        bar = jnp.max(jnp.where(kpos <= positions(yq, 0, lanes), sc, NEG_LARGE), axis=0, keepdims=True)
        st_ref[yq, 0:1] = bar
        st_ref[yq, 1:2] = bar * factor

    def tiles(yq, blocks, mask=None):
        keys = jnp.concatenate([k_all[b] for b in blocks], axis=0)
        vals = jnp.concatenate([v_all[b] for b in blocks], axis=1)
        depth = rows if len(blocks) == 1 else min(DEPTH, rows)
        work = [(at, low) for at in range(0, lanes, width) for low in range(0, keys.shape[0], depth)]

        def scores(item):
            at, low = item
            return jnp.dot(keys[low : low + depth], qz_ref[yq, :, at : at + width], preferred_element_type=F32)

        ahead = [scores(item) for item in work[:LEAD]]
        total, gain = None, None
        for i, (at, low) in enumerate(work):
            sc = ahead.pop(0)
            if i + LEAD < len(work):
                ahead.append(scores(work[i + LEAD]))
            cols = slice(at, at + width)
            expo = jnp.exp2(sc * factor - st_ref[yq, 1:2, cols])
            if mask is not None:
                expo = jnp.where(mask(at)[low : low + depth], expo, 0.0)
            part = jnp.sum(expo.reshape(depth // 8, 8, width), axis=0)
            total = part if low == 0 else total + part
            term = jnp.dot(vals[:, low : low + depth], expo.astype(BF16), preferred_element_type=F32)
            gain = term if low == 0 else gain + term
            if low + depth == keys.shape[0]:
                sum_ref[yq, :, cols] += total
                acc_ref[yq, :, cols] += gain

    def at_distance(j, yq):
        below = z >= j
        above = jnp.logical_and(z + j >= nz, 2 * j < nz)

        @pl.when(jnp.logical_and(below, above))
        def _():
            tiles(yq, [lax.rem(z + nz - j, nz), lax.rem(z + j, nz)])

        @pl.when(jnp.logical_xor(below, above))
        def _():
            tiles(yq, [lax.rem(jnp.where(below, z + nz - j, z + j), nz)])

    def query_block(i):
        away = (i + 1) // 2
        return lax.rem(y + jnp.where(i % 2 == 1, away, ny - away), ny)

    def first_visits(first, last):
        def visit(i, carry):
            yq = query_block(i)

            @pl.when(i > 0)
            def _():
                begin(yq)

                @pl.when(yq > y)
                def _():
                    tiles(yq, [z])

            at_distance(1, yq)
            return carry

        if first < last:
            lax.fori_loop(first, last, visit, 0)

    def later_visits(j):
        def visit(i, carry):
            at_distance(j, query_block(i))
            return carry

        lax.fori_loop(0, ny, visit, 0)

    begin(y)
    kpos = (z * ny + y) * rows + lax.broadcasted_iota(jnp.int32, (rows, 1), 0)
    tiles(y, [z], lambda at: kpos <= positions(y, at, width))
    sy, sz = ring_y.steps, ring_z.steps
    for k in range(1, min(sy, 2) + 1):
        ring_y.step(k)
    ring_z.step(1)
    here = min(ny, 2 * min(sy, 2) + 1)
    first_visits(0, min(3, here))
    if sy >= 3:
        ring_y.step(3)
    first_visits(3, here)
    if sz >= 2:
        ring_z.step(2)
    if sy >= 4:
        ring_y.step(4)
    shared.step(1, range(EARLY // 2))
    first_visits(here, ny)
    for j in range(2, sz + 1):
        if j < sz:
            ring_z.step(j + 1)
        if j + 1 == sz:
            shared.step(1, range(EARLY // 2, EARLY))
        later_visits(j)
    if sz < 3:
        shared.step(1, range(EARLY // 2, EARLY))
    shared.step(2, range(EARLY))
    for b in range(ny):
        st_ref[b, 1:2] = jnp.sum(sum_ref[b], axis=0, keepdims=True)
    hcopy.wait_recv()
    hcopy.wait_send()
    ring_z.finish()
    ring_y.finish()
    shared.finish()


def repair_kernel(ny, scale, q_all, k_all, v_all, acc_in, st_in, acc_ref, st_ref, qz_ref):
    s = lax.axis_index("sp")
    z, y = s // ny, s % ny
    rows = q_all.shape[2]
    half = q_all.shape[1] // 2
    lanes = 2 * rows
    factor = scale / math.log(2.0)
    calm = jnp.max(st_in[:, 1:2]) < 2.0**80

    @pl.when(calm)
    def _():
        acc_ref[...] = acc_in[...]
        st_ref[:, 0:2] = st_in[:, 0:2]

    @pl.when(jnp.logical_not(calm))
    def _():
        def slow(yq, carry):
            qt = q_all[yq]
            low = lax.broadcasted_iota(jnp.int32, qt.shape, 0) < half
            zero = jnp.zeros_like(qt)
            qz_ref[:, 0:rows] = jnp.where(low, qt, zero)
            qz_ref[:, rows:] = jnp.where(low, zero, qt)
            acc_ref[yq] = jnp.zeros((acc_ref.shape[1], lanes), F32)
            st_ref[yq, 0:1] = jnp.full((1, lanes), NEG_LARGE, F32)
            st_ref[yq, 1:2] = jnp.zeros((1, lanes), F32)

            def block(b, carry):
                kpos = (b * ny + y) * rows + lax.broadcasted_iota(jnp.int32, (rows, 1), 0)

                def group(g, carry):
                    at = pl.multiple_of(g * 128, 128)
                    cols = pl.ds(at, 128)
                    lane = lax.broadcasted_iota(jnp.int32, (1, 128), 1) + at
                    qpos = jnp.where(lane >= rows, lane - rows, lane) + (z * ny + yq) * rows
                    allowed = kpos <= qpos
                    sc = jnp.dot(k_all[b], qz_ref[:, cols], preferred_element_type=F32)
                    sc = jnp.where(allowed, sc, NEG_LARGE)
                    old = st_ref[yq, 0:1, cols]
                    new = jnp.maximum(old, jnp.max(sc, axis=0, keepdims=True))
                    expo = jnp.where(allowed, jnp.exp2((sc - new) * factor), 0.0)
                    shrink = jnp.exp2((old - new) * factor)
                    st_ref[yq, 0:1, cols] = new
                    st_ref[yq, 1:2, cols] = st_ref[yq, 1:2, cols] * shrink + jnp.sum(expo, axis=0, keepdims=True)
                    acc_ref[yq, :, cols] = acc_ref[yq, :, cols] * shrink + jnp.dot(
                        v_all[b], expo.astype(BF16), preferred_element_type=F32
                    )
                    return carry

                return lax.fori_loop(0, lanes // 128, group, carry)

            return lax.fori_loop(0, z + 1, block, carry)

        lax.fori_loop(0, ny, slow, 0)


def finish_kernel(
    ny, nx, scale, acc_ref, st_ref, lam_ref, gain_ref, p_ref, halo, gw_ref, ps_ref, wo_ref, late_ref, out_ref,
    mix, branch, wo_late, wbuf, sbuf, wland, sland, lands, ws, wr, ss, sr, xs, xr, ps, pr, os, or_,
):
    s, t = lax.axis_index("sp"), lax.axis_index("tp")
    z, y = s // ny, s % ny
    tp = 2 * nx
    rows, head = p_ref.shape
    orows = out_ref.shape[0]
    factor = scale / math.log(2.0)
    dev = lambda i: (z * ny + i % ny, t)
    shared = Shared(nx, late_ref, wo_late, PARTS - EARLY, late_ref.shape[0] // (PARTS - EARLY), xs, xr, ps, pr)
    others = [(s, (t + d) % tp) for d in range(1, tp)]
    greet([dev(y + 1), dev(y + ny - 1)] + others)

    def pooled():
        here = p_ref[...].astype(F32)
        rim = jnp.where(s > 0, halo[...].astype(F32), 0.0)
        total = jnp.concatenate([rim, here], axis=0)
        slot = t % 4
        for i in range(4):
            more = total + pltpu.roll(total, 1 << i, 0)
            total = jnp.where(i <= slot, more, total)
        span = jnp.where(slot == 0, 2, jnp.where(slot == 1, 4, jnp.where(slot == 2, 8, 16)))
        pos = s * rows + lax.broadcasted_iota(jnp.int32, (rows, 1), 0)
        count = jnp.minimum(pos + 1, span).astype(F32)
        differ = (total[RIM:] / count - here).astype(BF16)
        return (jnp.dot(differ, gw_ref[0], preferred_element_type=F32) * ps_ref[...]).astype(BF16)

    def own(block, m):
        cols = slice(m * rows, (m + 1) * rows)
        return acc_ref[block, :, cols], st_ref[block, 0:1, cols], st_ref[block, 1:2, cols]

    def joined(a, b):
        top = jnp.maximum(a[1], b[1])
        fa, fb = jnp.exp2((a[1] - top) * factor), jnp.exp2((b[1] - top) * factor)
        return a[0] * fa + b[0] * fb, top, a[2] * fa + b[2] * fb

    def landed(d, m, k):
        return wland[d, m, k].astype(F32), sland[d, m, k, 0:1], sland[d, m, k, 1:2]

    def copies(d, m, k):
        to = dev(y + (1 if d == 0 else ny - 1))
        return [
            rcopy(wbuf.at[d, m, k], wland.at[d, m, k], ws.at[d, m, k], wr.at[d, m, k], to),
            rcopy(sbuf.at[d, m, k], sland.at[d, m, k], ss.at[d, m, k], sr.at[d, m, k], to),
        ]

    for k in range(ny // 2):
        for m in range(2):
            for d in range(2):
                n = hops(ny, d, m)
                if k >= n:
                    continue
                sign = 1 if d == 0 else -1
                block = (y + sign * (n - k)) % ny
                state = own(block, m)
                if k > 0:
                    for copy in copies(d, m, k - 1):
                        copy.wait_recv()
                    state = joined(state, landed(d, m, k - 1))
                wbuf[d, m, k] = state[0].astype(BF16)
                sbuf[d, m, k, 0:1] = state[1]
                sbuf[d, m, k, 1:2] = state[2]
                for copy in copies(d, m, k):
                    copy.start()
        if k == 0:
            shared.start()
            branch[:, head:] = pooled()
        if k == min(2, ny // 2 - 1):
            shared.step(1, range(PARTS - EARLY))
    for m in range(2):
        state = own(y, m)
        for d in range(2):
            n = hops(ny, d, m)
            if n > 0:
                for copy in copies(d, m, n - 1):
                    copy.wait_recv()
                state = joined(state, landed(d, m, n - 1))
        if m == 0:
            mix[...] = state[0] / state[2]
        else:
            mix[...] = mix[...] - lam_ref[0:1, 0:1] * state[0] / state[2]
    mixed = mix[...]
    mean = jnp.mean(mixed * mixed, axis=0, keepdims=True)
    normed = jnp.transpose(mixed * lax.rsqrt(mean + EPSILON)) * gain_ref[...]
    branch[:, 0:head] = normed.astype(BF16)

    outs = []
    for d in range(1, tp):
        at = pl.multiple_of(((t + d) % tp) * orows, 16)
        outs.append(rcopy(branch.at[pl.ds(at, orows)], lands.at[t], os.at[d - 1], or_.at[d - 1], others[d - 1]))
        outs[-1].start()
    lands[t] = branch[pl.ds(pl.multiple_of(t * orows, 16), orows)]
    shared.step(2, range(PARTS - EARLY))
    shared.finish()
    for copy in outs:
        copy.wait_recv()
    at = 0
    for ref in (wo_ref, wo_late):
        step = math.gcd(512, ref.shape[1])
        for low in range(0, ref.shape[1], step):
            total = None
            for i in range(tp):
                term = lax.dot_general(
                    lands[i], ref[i, low : low + step], (((1,), (1,)), ((), ())), preferred_element_type=F32
                )
                total = term if total is None else total + term
            out_ref[:, at : at + step] = total.astype(BF16)
            at += step
    for copy in outs:
        copy.wait_send()
    for k in range(ny // 2):
        for m in range(2):
            for d in range(2):
                if k < hops(ny, d, m):
                    for copy in copies(d, m, k):
                        copy.wait_send()


def local(sp, tp, tokens, pre_gain, w_query, w_key, w_value, w_pool, lambdas, sub_gain, group_weight, pool_scale, w_out):
    nz, ny = grid_of(sp)
    nx = tp // 2
    rows, part = tokens.shape
    wrows = w_query.shape[0]
    head = w_value.shape[1]
    qd = w_query.shape[1]
    whole = 3 * qd + 3 * head
    ncols = sp * w_out.shape[1]
    early = ncols // PARTS * EARLY
    scale = 1.0 / math.sqrt(qd // 2)
    dma = pltpu.SemaphoreType.DMA
    tok_full, w_full = call(
        functools.partial(gather_kernel, nz, ny, nx),
        [
            pltpu.with_memory_space_constraint(a, pltpu.HBM)
            for a in (tokens, pre_gain.reshape(1, part), w_query, w_key, w_value, w_pool, w_out.T)
        ],
        (sds(tp, rows + 16, part), sds(nz, ny, 2, wrows // 2, whole)),
        [VMEM((rows + 16, part), BF16), VMEM((wrows, whole), BF16), VMEM((1, part), BF16), dma((7,))]
        + [dma((2 * nx,)), dma((2 * nx,)), dma((ny,)), dma((ny,)), dma((nz,)), dma((nz,))]
        + ring_sems(nz, 2)
        + ring_sems(ny, 2),
        cid=0,
        space=pltpu.HBM,
        name="gather",
    )
    qt, k, vt, pool, wo_early, wo_late = call(
        functools.partial(project_kernel, tp),
        (tok_full, w_full.reshape(sp * wrows, whole)),
        (sds(qd, rows), sds(rows, qd), sds(head, rows), sds(rows, head), sds(early, 2 * head), sds(ncols - early, 2 * head)),
        [VMEM((rows, tp * part), BF16), VMEM((rows, 128), F32)],
        name="project",
    )
    totals = (sds(ny, head, 2 * rows, dtype=F32), sds(ny, 8, 2 * rows, dtype=F32))
    q_all, k_all, v_all, halo, wo_all, acc, st = call(
        functools.partial(attend_kernel, nz, ny, nx, scale),
        (qt, k, vt, pool, wo_early),
        (sds(ny, qd, rows), sds(nz, rows, qd), sds(nz, head, rows), sds(RIM, head), sds(tp, early, 2 * head))
        + totals,
        [VMEM((ny, qd, 2 * rows), BF16), VMEM((ny, 8, 2 * rows), F32)]
        + ring_sems(nz, 2) + ring_sems(ny, 2) + shared_sems(nx, EARLY) + [dma, dma],
        cid=1,
        name="attend",
    )
    acc, st = call(
        functools.partial(repair_kernel, ny, scale),
        (q_all, k_all, v_all, acc, st),
        totals,
        [VMEM((qd, 2 * rows), BF16)],
        name="repair",
    )
    half = ny // 2
    orows = rows // tp
    (out,) = call(
        functools.partial(finish_kernel, ny, nx, scale),
        (
            acc,
            st,
            jnp.broadcast_to(lambdas.reshape(1, 1), (8, 128)),
            sub_gain.reshape(1, head),
            pool,
            halo,
            group_weight,
            pool_scale.reshape(1, head),
            wo_all,
            wo_late,
        ),
        (sds(orows, ncols),),
        [
            VMEM((head, rows), F32),
            VMEM((rows, 2 * head), BF16),
            VMEM((tp, ncols - early, 2 * head), BF16),
            VMEM((2, 2, half, head, rows), BF16),
            VMEM((2, 2, half, 8, rows), F32),
            VMEM((2, 2, half, head, rows), BF16),
            VMEM((2, 2, half, 8, rows), F32),
            VMEM((tp, orows, 2 * head), BF16),
        ]
        + [dma((2, 2, half))] * 4
        + shared_sems(nx, PARTS - EARLY)
        + [dma((tp,))] * 2,
        cid=2,
        name="finish",
    )
    return out


def solution(mesh):
    placed = (
        P("sp", "tp"),
        P("tp"),
        P("sp", "tp"),
        P("sp", "tp"),
        P("sp", "tp"),
        P("sp", "tp"),
        P("tp"),
        P(),
        P("tp", None, None),
        P("tp"),
        P("tp", "sp"),
    )
    body = functools.partial(local, mesh.shape["sp"], mesh.shape["tp"])
    return jax.shard_map(body, mesh=mesh, in_specs=placed, out_specs=P(("sp", "tp"), None), check_vma=False)
```

```python
import functools
import math

import jax
import jax.numpy as jnp
from jax import lax
from jax.experimental import pallas as pl
from jax.experimental.pallas import tpu as pltpu
from jax.sharding import PartitionSpec as P

MESH = pl.DeviceIdType.MESH
VMEM = pltpu.VMEM
EPSILON = 1e-06
NEG_LARGE = -1e30
F32, BF16 = jnp.float32, jnp.bfloat16
RIM = 16
LEAD = 1
PARTS = 8


def grid_of(sp):
    ny = 2 ** ((sp.bit_length() - 1) // 2)
    return sp // ny, ny


def vspec(n):
    return [pl.BlockSpec(memory_space=VMEM)] * n


def sds(*shape, dtype=BF16):
    return jax.ShapeDtypeStruct(shape, dtype)


def call(kernel, ins, outs, scratch=(), cid=None, limit=40 << 20, name=None, flops=1 << 24, space=VMEM):
    params = dict(vmem_limit_bytes=limit)
    if cid is not None:
        params.update(collective_id=cid, has_side_effects=True)
    return pl.pallas_call(
        kernel,
        out_shape=tuple(outs),
        in_specs=[pl.BlockSpec(memory_space=space)] * len(ins),
        out_specs=tuple(vspec(len(outs))),
        scratch_shapes=list(scratch),
        compiler_params=pltpu.CompilerParams(**params),
        cost_estimate=pl.CostEstimate(flops=flops, bytes_accessed=1 << 20, transcendentals=0),
        name=name,
    )(*ins)


def rcopy(src, dst, ssem, rsem, dev):
    return pltpu.make_async_remote_copy(
        src_ref=src, dst_ref=dst, send_sem=ssem, recv_sem=rsem, device_id=dev, device_id_type=MESH
    )


def greet(peers):
    barrier = pltpu.get_barrier_semaphore()
    for dev in peers:
        pl.semaphore_signal(barrier, inc=1, device_id=dev, device_id_type=MESH)
    pl.semaphore_wait(barrier, len(peers))


def hops(n, direction, sub):
    return n // 2 if (direction + sub) % 2 == 0 else (n - 1) // 2


class Ring:
    def __init__(self, n, me, dev, piece, subs, ssem, rsem):
        self.n, self.me, self.dev, self.piece, self.subs = n, me, dev, piece, subs
        self.ssem, self.rsem = ssem, rsem
        self.steps = n // 2

    def copy(self, d, sub, k):
        sign = 1 if d == 0 else -1
        block = (self.me - sign * k) % self.n
        ref = self.piece(block, sub)
        return rcopy(
            ref, ref, self.ssem.at[d, sub, k], self.rsem.at[d, sub, k], self.dev((self.me + sign) % self.n)
        )

    def step(self, k):
        for sub in range(self.subs):
            for d in range(2):
                if k > 0 and k - 1 < hops(self.n, d, sub):
                    self.copy(d, sub, k - 1).wait_recv()
                if k < hops(self.n, d, sub):
                    self.copy(d, sub, k).start()

    def open(self):
        for far in range(self.steps, 0, -1):
            for sub in range(self.subs):
                for d in range(2):
                    if hops(self.n, d, sub) == far:
                        self.copy(d, sub, 0).start()

    def pass_on(self, k, landed, onward):
        for sub in range(self.subs):
            for d in range(2):
                if k - 1 < hops(self.n, d, sub) and (k < hops(self.n, d, sub)) == onward:
                    self.copy(d, sub, k - 1).wait_recv()
                    if onward:
                        self.copy(d, sub, k).start()
                    landed((self.me + (k if d else -k)) % self.n, sub)

    def finish(self):
        for k in range(self.steps):
            for sub in range(self.subs):
                for d in range(2):
                    if k < hops(self.n, d, sub):
                        self.copy(d, sub, k).wait_send()


def ring_sems(n, subs):
    return [pltpu.SemaphoreType.DMA((2, subs, max(n // 2, 1))), pltpu.SemaphoreType.DMA((2, subs, max(n // 2, 1)))]


class Shared:
    def __init__(self, nx, own, buf, subs, size, rs, rr, ps, pr):
        s, t = lax.axis_index("sp"), lax.axis_index("tp")
        x, c = t // 2, t % 2
        self.nx, self.x, self.c, self.t = nx, x, c, t
        self.buf, self.ps, self.pr, self.own = buf, ps, pr, own
        self.partner = (s, x * 2 + 1 - c)
        self.peers = [(s, ((x + d) % nx) * 2 + c) for d in ((1, nx - 1) if nx > 1 else ())] + [self.partner]
        self.piece = lambda b, i: buf.at[2 * b + c, i * size : (i + 1) * size]
        self.ring = Ring(nx, x, lambda i: (s, 2 * i + c), self.piece, subs, rs, rr)
        self.subs = subs
        self.relays = []

    def relay(self, block, sub):
        ref = self.piece(block, sub)
        at = len(self.relays)
        copy = rcopy(ref, ref, self.ps.at[at], self.pr.at[at], self.partner)
        copy.start()
        self.relays.append(copy)

    def start(self):
        self.buf[self.t] = self.own[...]
        self.ring.open()
        self.direct = rcopy(
            self.own, self.buf.at[self.t], self.ps.at[self.subs * self.nx], self.pr.at[self.subs * self.nx], self.partner
        )
        self.direct.start()

    def step(self, k, onward):
        if k <= self.ring.steps:
            self.ring.pass_on(k, self.relay, onward)

    def finish(self):
        for copy in self.relays + [self.direct]:
            copy.wait_recv()
        for copy in self.relays + [self.direct]:
            copy.wait_send()
        self.ring.finish()


def shared_sems(nx, subs):
    dma = pltpu.SemaphoreType.DMA
    return ring_sems(nx, subs) + [dma((subs * nx + 1,)), dma((subs * nx + 1,))]


def gather_kernel(nz, ny, nx, tin_ref, gain_ref, wq_ref, wk_ref, wv_ref, wp_ref, wo_ref, tok_full, w_full, tok_ref, w_ref, gain, ins, ts, tr, ys, yr, zs, zr, as_, ar, bs, br):
    s, t = lax.axis_index("sp"), lax.axis_index("tp")
    z, y, x, c = s // ny, s % ny, t // 2, t % 2
    half = w_ref.shape[0] // 2
    rows = tin_ref.shape[0]
    loads = [pltpu.make_async_copy(tin_ref, tok_ref.at[0:rows], ins.at[0]), pltpu.make_async_copy(gain_ref, gain, ins.at[1])]
    at = 0
    for i, ref in enumerate((wq_ref, wk_ref, wv_ref, wp_ref, wo_ref)):
        loads.append(pltpu.make_async_copy(ref, w_ref.at[:, at : at + ref.shape[1]], ins.at[2 + i]))
        at += ref.shape[1]
    for load in loads:
        load.start()
    loads[1].wait()
    tok_ref[rows:] = jnp.broadcast_to(gain[...], (16, gain.shape[1]))
    partner = (s, x * 2 + 1 - c)
    across = [(s, ((x + d) % nx) * 2 + c) for d in range(1, nx)]
    along_y = [(z * ny + (y + d) % ny, t) for d in range(1, ny)]
    along_z = [(((z + d) % nz) * ny + y, t) for d in range(1, nz)]
    greet([partner] + across + along_y + along_z)
    for i, load in enumerate(loads):
        if i != 1:
            load.wait()

    ysends = [
        rcopy(w_ref.at[0:half], w_full.at[z, y, 0], ys.at[d], yr.at[d], along_y[d]) for d in range(ny - 1)
    ]
    zsends = [
        rcopy(w_ref.at[half:], w_full.at[z, y, 1], zs.at[d], zr.at[d], along_z[d]) for d in range(nz - 1)
    ]
    tsends = [rcopy(tok_ref, tok_full.at[t], ts.at[d], tr.at[d], across[d]) for d in range(nx - 1)]
    tsends.append(rcopy(tok_ref, tok_full.at[t], ts.at[nx - 1], tr.at[nx - 1], partner))
    for copy in ysends + zsends + tsends:
        copy.start()
    w_full[z, y, 0] = w_ref[0:half]
    w_full[z, y, 1] = w_ref[half:]
    tok_full[t] = tok_ref[...]

    def piece_a(block, sub):
        return w_full.at[block, sub * (ny // 2) : (sub + 1) * (ny // 2), 0]

    def piece_b(block, sub):
        return w_full.at[sub * (nz // 2) : (sub + 1) * (nz // 2), block, 1]

    ring_a = Ring(nz, z, lambda i: (i * ny + y, t), piece_a, 2, as_, ar)
    ring_b = Ring(ny, y, lambda i: (z * ny + i, t), piece_b, 2, bs, br)
    for copy in ysends:
        copy.wait_recv()
    ring_a.step(0)
    for copy in zsends:
        copy.wait_recv()
    ring_b.step(0)
    relays = []
    for k in range(1, max(ring_a.steps, ring_b.steps) + 1):
        if k <= ring_a.steps:
            ring_a.step(k)
        if k <= ring_b.steps:
            ring_b.step(k)
        if k == 1:
            for d in range(nx - 1):
                tsends[d].wait_recv()
                source = ((x - 1 - d) % nx) * 2 + c
                relays.append(
                    rcopy(tok_full.at[source], tok_full.at[source], ts.at[nx + d], tr.at[nx + d], partner)
                )
                relays[-1].start()
    tsends[-1].wait_recv()
    for copy in relays:
        copy.wait_recv()
    for copy in ysends + zsends + tsends + relays:
        copy.wait_send()
    ring_a.finish()
    ring_b.finish()


def project_kernel(tp, tok_ref, w_ref, qt_ref, k_ref, vt_ref, pool_ref, wo_ref, scaled, sq):
    rows, part = qt_ref.shape[1], tok_ref.shape[2]
    wo_ref[...] = w_ref[:, 512:]
    sq[...] = jnp.zeros_like(sq)
    for t in range(tp):
        x = tok_ref[t, 0:rows].astype(F32)
        gain = tok_ref[t, rows : rows + 1].astype(F32)
        squares = x * x
        for i in range(part // 128):
            sq[...] += squares[:, i * 128 : (i + 1) * 128]
        scaled[:, t * part : (t + 1) * part] = (x * gain).astype(BF16)
    inverse = lax.rsqrt(jnp.sum(sq[...], axis=1, keepdims=True) / (tp * part) + EPSILON)

    def project(at):
        out = jnp.dot(scaled[...], w_ref[:, at * 128 : at * 128 + 256], preferred_element_type=F32) * inverse
        return out[:, 0:128].astype(BF16), out[:, 128:256].astype(BF16)

    q, k = project(0)
    qt_ref[...] = jnp.transpose(q.astype(F32)).astype(BF16)
    k_ref[...] = k
    v, p = project(2)
    vt_ref[...] = jnp.transpose(v.astype(F32)).astype(BF16)
    pool_ref[...] = p


def attend_kernel(
    nz, ny, nx, scale, q_ref, k_ref, v_ref, p_ref, wo_ref, lam_ref, gain_ref, gw_ref, ps_ref, out_ref,
    q_all, k_all, v_all, halo, wo_all, acc_ref, st_ref, qz_ref, sum_ref, mix, branch, wbuf, sbuf, wland, sland, lands,
    zs, zr, ys, yr, xs, xr, ps, pr, hs, hr, ms, mr, ss, sr, os, or_,
):
    head = p_ref.shape[1]
    orows = out_ref.shape[0]
    s, t = lax.axis_index("sp"), lax.axis_index("tp")
    z, y = s // ny, s % ny
    sp = nz * ny
    dev_z = lambda i: (i * ny + y, t)
    dev_y = lambda i: (z * ny + i, t)
    rows = p_ref.shape[0]
    nxt, prv = ((s + 1) % sp, t), ((s + sp - 1) % sp, t)
    shared = Shared(nx, wo_ref, wo_all, PARTS, wo_ref.shape[0] // PARTS, xs, xr, ps, pr)
    tp = 2 * nx
    others = [(s, (t + d) % tp) for d in range(1, tp)]
    near = [dev_z((z + 1) % nz), dev_z((z + nz - 1) % nz), dev_y((y + 1) % ny), dev_y((y + ny - 1) % ny)]
    greet(near + [nxt, prv] + others)
    q_all[y] = q_ref[...]
    k_all[z] = k_ref[...]
    v_all[z] = v_ref[...]
    half = q_ref.shape[0] // 2
    ring_y = Ring(ny, y, dev_y, lambda b, i: q_all.at[b, i * half : (i + 1) * half], 2, ys, yr)
    ring_z = Ring(nz, z, dev_z, lambda b, i: (k_all if i == 0 else v_all).at[b], 2, zs, zr)
    ring_y.step(0)
    ring_z.step(0)
    shared.start()
    hcopy = rcopy(p_ref.at[rows - RIM :], halo, hs, hr, nxt)
    hcopy.start()

    lanes = 2 * rows
    width = min(256, rows)
    vd = v_all.shape[1]
    factor = scale / math.log(2.0)

    def positions(yq, at, wide):
        lane = lax.broadcasted_iota(jnp.int32, (1, wide), 1) + at
        return jnp.where(lane >= rows, lane - rows, lane) + (z * ny + yq) * rows

    def begin(yq):
        qt = q_all[yq]
        low = lax.broadcasted_iota(jnp.int32, qt.shape, 0) < half
        zero = jnp.zeros_like(qt)
        qz_ref[yq, :, 0:rows] = jnp.where(low, qt, zero)
        qz_ref[yq, :, rows:] = jnp.where(low, zero, qt)
        acc_ref[yq] = jnp.zeros((vd, lanes), F32)
        sum_ref[yq] = jnp.zeros((8, lanes), F32)
        st_ref[yq, 0:1] = jnp.full((1, lanes), NEG_LARGE, F32)

    def tiles(yq, blocks, mask=None):
        keys = jnp.concatenate([k_all[b] for b in blocks], axis=0)
        vals = jnp.concatenate([v_all[b] for b in blocks], axis=1)
        depth = keys.shape[0]
        work = list(range(0, lanes, width))

        def scores(at):
            sc = jnp.dot(keys, qz_ref[yq, :, at : at + width], preferred_element_type=F32)
            if mask is not None:
                sc = jnp.where(mask(at), sc, NEG_LARGE)
            return sc, jnp.max(sc, axis=0, keepdims=True)

        ahead = [scores(at) for at in work[:LEAD]]
        for i, at in enumerate(work):
            sc, top = ahead.pop(0)
            if i + LEAD < len(work):
                ahead.append(scores(work[i + LEAD]))
            cols = slice(at, at + width)
            old = st_ref[yq, 0:1, cols]
            new = jnp.maximum(old, top)
            expo = jnp.exp2(sc * factor - new * factor)
            if mask is not None:
                expo = jnp.where(mask(at), expo, 0.0)
            shrink = jnp.exp2((old - new) * factor)
            st_ref[yq, 0:1, cols] = new
            part = jnp.sum(expo.reshape(depth // 8, 8, width), axis=0)
            sum_ref[yq, :, cols] = sum_ref[yq, :, cols] * shrink + part
            term = jnp.dot(vals, expo.astype(BF16), preferred_element_type=F32)
            acc_ref[yq, :, cols] = acc_ref[yq, :, cols] * shrink + term

    def at_distance(j, yq):
        below = z >= j
        above = jnp.logical_and(z + j >= nz, 2 * j < nz)

        @pl.when(jnp.logical_and(below, above))
        def _():
            tiles(yq, [lax.rem(z + nz - j, nz), lax.rem(z + j, nz)])

        @pl.when(jnp.logical_xor(below, above))
        def _():
            tiles(yq, [lax.rem(jnp.where(below, z + nz - j, z + j), nz)])

    def query_block(i):
        away = (i + 1) // 2
        return lax.rem(y + jnp.where(i % 2 == 1, away, ny - away), ny)

    def first_visits(first, last):
        def visit(i, carry):
            yq = query_block(i)

            @pl.when(i > 0)
            def _():
                begin(yq)

                @pl.when(yq > y)
                def _():
                    tiles(yq, [z])

            at_distance(1, yq)
            return carry

        if first < last:
            lax.fori_loop(first, last, visit, 0)

    def complete(first, last):
        def visit(i, carry):
            def near(j, carry):
                at_distance(j, query_block(i))
                return carry

            return lax.fori_loop(2, ring_z.steps + 1, near, carry)

        if first < last and ring_z.steps > 1:
            lax.fori_loop(first, last, visit, 0)

    begin(y)
    kpos = (z * ny + y) * rows + lax.broadcasted_iota(jnp.int32, (rows, 1), 0)
    tiles(y, [z], lambda at: kpos <= positions(y, at, width))
    sy, sz = ring_y.steps, ring_z.steps
    for k in range(1, min(sy, 2) + 1):
        ring_y.step(k)
    ring_z.step(1)
    here = min(ny, 2 * min(sy, 2) + 1)
    near_end, far_end = min(3, here), max(here, ny - 2)
    first_visits(0, near_end)
    if sz >= 2:
        ring_z.step(2)
    if sy >= 3:
        ring_y.step(3)
    first_visits(near_end, here)
    if sy >= 4:
        ring_y.step(4)
    first_visits(here, far_end)
    if sz >= 3:
        ring_z.step(3)
    shared.step(1, True)
    first_visits(far_end, ny)
    if sz >= 4:
        ring_z.step(4)

    def pooled():
        here = p_ref[...].astype(F32)
        rim = jnp.where(s > 0, halo[...].astype(F32), 0.0)
        total = jnp.concatenate([rim, here], axis=0)
        slot = t % 4
        for i in range(4):
            more = total + pltpu.roll(total, 1 << i, 0)
            total = jnp.where(i <= slot, more, total)
        span = jnp.where(slot == 0, 2, jnp.where(slot == 1, 4, jnp.where(slot == 2, 8, 16)))
        pos = s * rows + lax.broadcasted_iota(jnp.int32, (rows, 1), 0)
        count = jnp.minimum(pos + 1, span).astype(F32)
        differ = (total[RIM:] / count - here).astype(BF16)
        return (jnp.dot(differ, gw_ref[0], preferred_element_type=F32) * ps_ref[...]).astype(BF16)

    def own(block, m):
        cols = slice(m * rows, (m + 1) * rows)
        return acc_ref[block, :, cols], st_ref[block, 0:1, cols], jnp.sum(sum_ref[block, :, cols], axis=0, keepdims=True)

    def joined(a, b):
        top = jnp.maximum(a[1], b[1])
        fa, fb = jnp.exp2((a[1] - top) * factor), jnp.exp2((b[1] - top) * factor)
        return a[0] * fa + b[0] * fb, top, a[2] * fa + b[2] * fb

    def landed(d, m, k):
        return wland[d, m, k].astype(F32), sland[d, m, k, 0:1], sland[d, m, k, 1:2]

    def copies(d, m, k):
        to = dev_y((y + (1 if d == 0 else ny - 1)) % ny)
        return [
            rcopy(wbuf.at[d, m, k], wland.at[d, m, k], ms.at[d, m, k], mr.at[d, m, k], to),
            rcopy(sbuf.at[d, m, k], sland.at[d, m, k], ss.at[d, m, k], sr.at[d, m, k], to),
        ]

    done = ny
    for k in range(ny // 2):
        complete(max(ny - 3 - 2 * k, 0), done)
        done = max(ny - 3 - 2 * k, 0)
        for m in range(2):
            for d in range(2):
                n = hops(ny, d, m)
                if k >= n:
                    continue
                sign = 1 if d == 0 else -1
                block = (y + sign * (n - k)) % ny
                state = own(block, m)
                if k > 0:
                    for copy in copies(d, m, k - 1):
                        copy.wait_recv()
                    state = joined(state, landed(d, m, k - 1))
                wbuf[d, m, k] = state[0].astype(BF16)
                sbuf[d, m, k, 0:1] = state[1]
                sbuf[d, m, k, 1:2] = state[2]
                for copy in copies(d, m, k):
                    copy.start()
        if k == 0:
            hcopy.wait_recv()
            branch[:, head:] = pooled()
    for m in range(2):
        state = own(y, m)
        for d in range(2):
            n = hops(ny, d, m)
            if n > 0:
                for copy in copies(d, m, n - 1):
                    copy.wait_recv()
                state = joined(state, landed(d, m, n - 1))
        if m == 0:
            mix[...] = state[0] / state[2]
        else:
            mix[...] = mix[...] - lam_ref[0:1, 0:1] * state[0] / state[2]
    mixed = mix[...]
    mean = jnp.mean(mixed * mixed, axis=0, keepdims=True)
    normed = jnp.transpose(mixed * lax.rsqrt(mean + EPSILON)) * gain_ref[...]
    branch[:, 0:head] = normed.astype(BF16)

    outs = []
    for d in range(1, tp):
        at = pl.multiple_of(((t + d) % tp) * orows, 16)
        outs.append(rcopy(branch.at[pl.ds(at, orows)], lands.at[t], os.at[d - 1], or_.at[d - 1], others[d - 1]))
        outs[-1].start()
    lands[t] = branch[pl.ds(pl.multiple_of(t * orows, 16), orows)]
    shared.step(1, False)
    shared.step(2, False)
    shared.finish()
    for copy in outs:
        copy.wait_recv()
    at = 0
    for ref in (wo_all,):
        step = math.gcd(512, ref.shape[1])
        for low in range(0, ref.shape[1], step):
            total = None
            for i in range(tp):
                term = lax.dot_general(
                    lands[i], ref[i, low : low + step], (((1,), (1,)), ((), ())), preferred_element_type=F32
                )
                total = term if total is None else total + term
            out_ref[:, at : at + step] = total.astype(BF16)
            at += step
    for copy in outs:
        copy.wait_send()
    for k in range(ny // 2):
        for m in range(2):
            for d in range(2):
                if k < hops(ny, d, m):
                    for copy in copies(d, m, k):
                        copy.wait_send()
    hcopy.wait_send()
    ring_z.finish()
    ring_y.finish()


def local(sp, tp, tokens, pre_gain, w_query, w_key, w_value, w_pool, lambdas, sub_gain, group_weight, pool_scale, w_out):
    nz, ny = grid_of(sp)
    nx = tp // 2
    rows, part = tokens.shape
    wrows = w_query.shape[0]
    head = w_value.shape[1]
    qd = w_query.shape[1]
    whole = 3 * qd + 3 * head
    ncols = sp * w_out.shape[1]
    scale = 1.0 / math.sqrt(qd // 2)
    dma = pltpu.SemaphoreType.DMA
    tok_full, w_full = call(
        functools.partial(gather_kernel, nz, ny, nx),
        [
            pltpu.with_memory_space_constraint(a, pltpu.HBM)
            for a in (tokens, pre_gain.reshape(1, part), w_query, w_key, w_value, w_pool, w_out.T)
        ],
        (sds(tp, rows + 16, part), sds(nz, ny, 2, wrows // 2, whole)),
        [VMEM((rows + 16, part), BF16), VMEM((wrows, whole), BF16), VMEM((1, part), BF16), dma((7,))]
        + [dma((2 * nx,)), dma((2 * nx,)), dma((ny,)), dma((ny,)), dma((nz,)), dma((nz,))]
        + ring_sems(nz, 2)
        + ring_sems(ny, 2),
        cid=0,
        space=pltpu.HBM,
        name="gather",
    )
    qt, k, vt, pool, wo = call(
        functools.partial(project_kernel, tp),
        (tok_full, w_full.reshape(sp * wrows, whole)),
        (sds(qd, rows), sds(rows, qd), sds(head, rows), sds(rows, head), sds(ncols, 2 * head)),
        [VMEM((rows, tp * part), BF16), VMEM((rows, 128), F32)],
        name="project",
    )
    half = ny // 2
    orows = rows // tp
    (out,) = call(
        functools.partial(attend_kernel, nz, ny, nx, scale),
        (
            qt,
            k,
            vt,
            pool,
            wo,
            jnp.broadcast_to(lambdas.reshape(1, 1), (8, 128)),
            sub_gain.reshape(1, head),
            group_weight,
            pool_scale.reshape(1, head),
        ),
        (sds(orows, ncols),),
        [
            VMEM((ny, qd, rows), BF16),
            VMEM((nz, rows, qd), BF16),
            VMEM((nz, head, rows), BF16),
            VMEM((RIM, head), BF16),
            VMEM((tp, ncols, 2 * head), BF16),
            VMEM((ny, head, 2 * rows), F32),
            VMEM((ny, 8, 2 * rows), F32),
            VMEM((ny, qd, 2 * rows), BF16),
            VMEM((ny, 8, 2 * rows), F32),
            VMEM((head, rows), F32),
            VMEM((rows, 2 * head), BF16),
            VMEM((2, 2, half, head, rows), BF16),
            VMEM((2, 2, half, 2, rows), F32),
            VMEM((2, 2, half, head, rows), BF16),
            VMEM((2, 2, half, 2, rows), F32),
            VMEM((tp, orows, 2 * head), BF16),
        ]
        + ring_sems(nz, 2)
        + ring_sems(ny, 2)
        + shared_sems(nx, PARTS)
        + [dma, dma]
        + [dma((2, 2, half))] * 4
        + [dma((tp,))] * 2,
        cid=1,
        name="attend",
    )
    return out


def solution(mesh):
    placed = (
        P("sp", "tp"),
        P("tp"),
        P("sp", "tp"),
        P("sp", "tp"),
        P("sp", "tp"),
        P("sp", "tp"),
        P("tp"),
        P(),
        P("tp", None, None),
        P("tp"),
        P("tp", "sp"),
    )
    body = functools.partial(local, mesh.shape["sp"], mesh.shape["tp"])
    return jax.shard_map(body, mesh=mesh, in_specs=placed, out_specs=P(("sp", "tp"), None), check_vma=False)
```

```python
import functools
import math

import jax
import jax.numpy as jnp
from jax import lax
from jax.experimental import pallas as pl
from jax.experimental.pallas import tpu as pltpu
from jax.sharding import PartitionSpec as P

MESH = pl.DeviceIdType.MESH
VMEM = pltpu.VMEM
EPSILON = 1e-06
NEG_LARGE = -1e30
F32, BF16 = jnp.float32, jnp.bfloat16
RIM = 16
LEAD = 1
PARTS = 8


def grid_of(sp):
    ny = 2 ** ((sp.bit_length() - 1) // 2)
    return sp // ny, ny


def vspec(n):
    return [pl.BlockSpec(memory_space=VMEM)] * n


def sds(*shape, dtype=BF16):
    return jax.ShapeDtypeStruct(shape, dtype)


def call(kernel, ins, outs, scratch=(), cid=None, limit=40 << 20, name=None, flops=1 << 24, space=()):
    params = dict(vmem_limit_bytes=limit)
    if cid is not None:
        params.update(collective_id=cid, has_side_effects=True)
    return pl.pallas_call(
        kernel,
        out_shape=tuple(outs),
        in_specs=[pl.BlockSpec(memory_space=one) for one in space],
        out_specs=tuple(vspec(len(outs))),
        scratch_shapes=list(scratch),
        compiler_params=pltpu.CompilerParams(**params),
        cost_estimate=pl.CostEstimate(flops=flops, bytes_accessed=1 << 20, transcendentals=0),
        name=name,
    )(*ins)


def rcopy(src, dst, ssem, rsem, dev):
    return pltpu.make_async_remote_copy(
        src_ref=src, dst_ref=dst, send_sem=ssem, recv_sem=rsem, device_id=dev, device_id_type=MESH
    )


def greet(peers):
    barrier = pltpu.get_barrier_semaphore()
    for dev in peers:
        pl.semaphore_signal(barrier, inc=1, device_id=dev, device_id_type=MESH)
    pl.semaphore_wait(barrier, len(peers))


def hops(n, direction, sub):
    return n // 2 if (direction + sub) % 2 == 0 else (n - 1) // 2


class Ring:
    def __init__(self, n, me, dev, piece, subs, ssem, rsem):
        self.n, self.me, self.dev, self.piece, self.subs = n, me, dev, piece, subs
        self.ssem, self.rsem = ssem, rsem
        self.steps = n // 2

    def copy(self, d, sub, k):
        sign = 1 if d == 0 else -1
        block = (self.me - sign * k) % self.n
        ref = self.piece(block, sub)
        return rcopy(
            ref, ref, self.ssem.at[d, sub, k], self.rsem.at[d, sub, k], self.dev((self.me + sign) % self.n)
        )

    def step(self, k):
        for sub in range(self.subs):
            for d in range(2):
                if k > 0 and k - 1 < hops(self.n, d, sub):
                    self.copy(d, sub, k - 1).wait_recv()
                if k < hops(self.n, d, sub):
                    self.copy(d, sub, k).start()

    def open(self):
        for far in range(self.steps, 0, -1):
            for sub in range(self.subs):
                for d in range(2):
                    if hops(self.n, d, sub) == far:
                        self.copy(d, sub, 0).start()

    def pass_on(self, k, landed, onward):
        for sub in range(self.subs):
            for d in range(2):
                if k - 1 < hops(self.n, d, sub) and (k < hops(self.n, d, sub)) == onward:
                    self.copy(d, sub, k - 1).wait_recv()
                    if onward:
                        self.copy(d, sub, k).start()
                    landed((self.me + (k if d else -k)) % self.n, sub)

    def finish(self):
        for k in range(self.steps):
            for sub in range(self.subs):
                for d in range(2):
                    if k < hops(self.n, d, sub):
                        self.copy(d, sub, k).wait_send()


def ring_sems(n, subs):
    return [pltpu.SemaphoreType.DMA((2, subs, max(n // 2, 1))), pltpu.SemaphoreType.DMA((2, subs, max(n // 2, 1)))]


class Shared:
    def __init__(self, nx, own, buf, subs, size, rs, rr, ps, pr):
        s, t = lax.axis_index("sp"), lax.axis_index("tp")
        x, c = t // 2, t % 2
        self.nx, self.x, self.c, self.t = nx, x, c, t
        self.buf, self.ps, self.pr, self.own = buf, ps, pr, own
        self.partner = (s, x * 2 + 1 - c)
        self.peers = [(s, ((x + d) % nx) * 2 + c) for d in ((1, nx - 1) if nx > 1 else ())] + [self.partner]
        self.piece = lambda b, i: buf.at[2 * b + c, i * size : (i + 1) * size]
        self.ring = Ring(nx, x, lambda i: (s, 2 * i + c), self.piece, subs, rs, rr)
        self.subs = subs
        self.relays = []

    def relay(self, block, sub):
        ref = self.piece(block, sub)
        at = len(self.relays)
        copy = rcopy(ref, ref, self.ps.at[at], self.pr.at[at], self.partner)
        copy.start()
        self.relays.append(copy)

    def start(self):
        self.buf[self.t] = self.own[...]
        self.ring.open()
        self.direct = rcopy(
            self.own, self.buf.at[self.t], self.ps.at[self.subs * self.nx], self.pr.at[self.subs * self.nx], self.partner
        )
        self.direct.start()

    def step(self, k, onward):
        if k <= self.ring.steps:
            self.ring.pass_on(k, self.relay, onward)

    def finish(self):
        for copy in self.relays + [self.direct]:
            copy.wait_recv()
        for copy in self.relays + [self.direct]:
            copy.wait_send()
        self.ring.finish()


def shared_sems(nx, subs):
    dma = pltpu.SemaphoreType.DMA
    return ring_sems(nx, subs) + [dma((subs * nx + 1,)), dma((subs * nx + 1,))]


def layer_kernel(
    nz, ny, nx, scale, tin_ref, gain_ref, wq_ref, wk_ref, wv_ref, wp_ref, wot_ref, lam_ref, sub_ref, gw_ref, ps_ref, out_ref,
    tok_ref, w_ref, gain, tok_full, w_full, scaled, sq, p_ref, wo_ref,
    q_all, k_all, v_all, halo, wo_all, acc_ref, st_ref, qz_ref, sum_ref, mix, branch, wbuf, sbuf, wland, sland, lands,
    ins, ts, tr, ys, yr, zs, zr, ga_s, ga_r, gb_s, gb_r,
    ks, kr, qs, qr, xs, xr, ps, pr, hs, hr, ms, mr, ss, sr, os, or_,
):
    orows = out_ref.shape[0]
    s, t = lax.axis_index("sp"), lax.axis_index("tp")
    z, y, x, c = s // ny, s % ny, t // 2, t % 2
    half = w_ref.shape[0] // 2
    rows, part = tin_ref.shape
    qd, head = wq_ref.shape[1], wv_ref.shape[1]
    sp, tp = nz * ny, 2 * nx
    loads = [pltpu.make_async_copy(tin_ref, tok_ref.at[0:rows], ins.at[0]), pltpu.make_async_copy(gain_ref, gain, ins.at[1])]
    at = 0
    for i, ref in enumerate((wq_ref, wk_ref, wv_ref, wp_ref, wot_ref)):
        loads.append(pltpu.make_async_copy(ref, w_ref.at[:, at : at + ref.shape[1]], ins.at[2 + i]))
        at += ref.shape[1]
    for load in loads:
        load.start()
    loads[1].wait()
    tok_ref[rows:] = jnp.broadcast_to(gain[...], (16, gain.shape[1]))
    partner = (s, x * 2 + 1 - c)
    across = [(s, ((x + d) % nx) * 2 + c) for d in range(1, nx)]
    along_y = [(z * ny + (y + d) % ny, t) for d in range(1, ny)]
    along_z = [(((z + d) % nz) * ny + y, t) for d in range(1, nz)]
    dev_z = lambda i: (i * ny + y, t)
    dev_y = lambda i: (z * ny + i, t)
    nxt, prv = ((s + 1) % sp, t), ((s + sp - 1) % sp, t)
    others = [(s, (t + d) % tp) for d in range(1, tp)]
    greet(others + along_y + along_z + [nxt, prv])
    for i, load in enumerate(loads):
        if i != 1:
            load.wait()

    ysends = [
        rcopy(w_ref.at[0:half], w_full.at[z, y, 0], ys.at[d], yr.at[d], along_y[d]) for d in range(ny - 1)
    ]
    zsends = [
        rcopy(w_ref.at[half:], w_full.at[z, y, 1], zs.at[d], zr.at[d], along_z[d]) for d in range(nz - 1)
    ]
    tsends = [rcopy(tok_ref, tok_full.at[t], ts.at[d], tr.at[d], across[d]) for d in range(nx - 1)]
    tsends.append(rcopy(tok_ref, tok_full.at[t], ts.at[nx - 1], tr.at[nx - 1], partner))
    for copy in ysends + zsends + tsends:
        copy.start()
    w_full[z, y, 0] = w_ref[0:half]
    w_full[z, y, 1] = w_ref[half:]
    tok_full[t] = tok_ref[...]

    def piece_a(block, sub):
        return w_full.at[block, sub * (ny // 2) : (sub + 1) * (ny // 2), 0]

    def piece_b(block, sub):
        return w_full.at[sub * (nz // 2) : (sub + 1) * (nz // 2), block, 1]

    ring_a = Ring(nz, z, lambda i: (i * ny + y, t), piece_a, 2, ga_s, ga_r)
    ring_b = Ring(ny, y, lambda i: (z * ny + i, t), piece_b, 2, gb_s, gb_r)
    for copy in ysends:
        copy.wait_recv()
    ring_a.step(0)
    for copy in zsends:
        copy.wait_recv()
    ring_b.step(0)
    relays = []
    for k in range(1, max(ring_a.steps, ring_b.steps) + 1):
        if k <= ring_a.steps:
            ring_a.step(k)
        if k <= ring_b.steps:
            ring_b.step(k)
        if k == 1:
            for d in range(nx - 1):
                tsends[d].wait_recv()
                source = ((x - 1 - d) % nx) * 2 + c
                relays.append(
                    rcopy(tok_full.at[source], tok_full.at[source], ts.at[nx + d], tr.at[nx + d], partner)
                )
                relays[-1].start()
    tsends[-1].wait_recv()
    for copy in relays:
        copy.wait_recv()
    for copy in ysends + zsends + tsends + relays:
        copy.wait_send()
    ring_a.finish()
    ring_b.finish()
    wo_ref[...] = w_full[:, :, :, :, 512:].reshape(wo_ref.shape)
    sq[...] = jnp.zeros_like(sq)
    for i in range(tp):
        values = tok_full[i, 0:rows].astype(F32)
        weight = tok_full[i, rows : rows + 1].astype(F32)
        squares = values * values
        for lane in range(0, part, 128):
            sq[...] += squares[:, lane : lane + 128]
        scaled[:, i * part : (i + 1) * part] = (values * weight).astype(BF16)
    inverse = lax.rsqrt(jnp.sum(sq[...], axis=1, keepdims=True) / (tp * part) + EPSILON)

    def project(at):
        out = jnp.dot(scaled[...], w_full[:, :, :, :, at * 128 : at * 128 + 256].reshape(tp * part, 256), preferred_element_type=F32) * inverse
        return out[:, 0:128].astype(BF16), out[:, 128:256].astype(BF16)

    q, k = project(0)
    q_all[y] = jnp.transpose(q.astype(F32)).astype(BF16)
    k_all[z] = k
    v, p = project(2)
    v_all[z] = jnp.transpose(v.astype(F32)).astype(BF16)
    p_ref[...] = p
    shared = Shared(nx, wo_ref, wo_all, PARTS, wo_ref.shape[0] // PARTS, xs, xr, ps, pr)
    half = qd // 2
    ring_y = Ring(ny, y, dev_y, lambda b, i: q_all.at[b, i * half : (i + 1) * half], 2, qs, qr)
    ring_z = Ring(nz, z, dev_z, lambda b, i: (k_all if i == 0 else v_all).at[b], 2, ks, kr)
    ring_y.step(0)
    ring_z.step(0)
    shared.start()
    hcopy = rcopy(p_ref.at[rows - RIM :], halo, hs, hr, nxt)
    hcopy.start()

    lanes = 2 * rows
    width = min(256, rows)
    vd = v_all.shape[1]
    factor = scale / math.log(2.0)

    def positions(yq, at, wide):
        lane = lax.broadcasted_iota(jnp.int32, (1, wide), 1) + at
        return jnp.where(lane >= rows, lane - rows, lane) + (z * ny + yq) * rows

    def begin(yq):
        qt = q_all[yq]
        low = lax.broadcasted_iota(jnp.int32, qt.shape, 0) < half
        zero = jnp.zeros_like(qt)
        qz_ref[yq, :, 0:rows] = jnp.where(low, qt, zero)
        qz_ref[yq, :, rows:] = jnp.where(low, zero, qt)
        acc_ref[yq] = jnp.zeros((vd, lanes), F32)
        sum_ref[yq] = jnp.zeros((8, lanes), F32)
        st_ref[yq, 0:1] = jnp.full((1, lanes), NEG_LARGE, F32)

    def tiles(yq, blocks, mask=None):
        keys = jnp.concatenate([k_all[b] for b in blocks], axis=0)
        vals = jnp.concatenate([v_all[b] for b in blocks], axis=1)
        depth = keys.shape[0]
        work = list(range(0, lanes, width))

        def scores(at):
            sc = jnp.dot(keys, qz_ref[yq, :, at : at + width], preferred_element_type=F32)
            if mask is not None:
                sc = jnp.where(mask(at), sc, NEG_LARGE)
            return sc, jnp.max(sc, axis=0, keepdims=True)

        ahead = [scores(at) for at in work[:LEAD]]
        for i, at in enumerate(work):
            sc, top = ahead.pop(0)
            if i + LEAD < len(work):
                ahead.append(scores(work[i + LEAD]))
            cols = slice(at, at + width)
            old = st_ref[yq, 0:1, cols]
            new = jnp.maximum(old, top)
            expo = jnp.exp2(sc * factor - new * factor)
            if mask is not None:
                expo = jnp.where(mask(at), expo, 0.0)
            shrink = jnp.exp2((old - new) * factor)
            st_ref[yq, 0:1, cols] = new
            part = jnp.sum(expo.reshape(depth // 8, 8, width), axis=0)
            sum_ref[yq, :, cols] = sum_ref[yq, :, cols] * shrink + part
            term = jnp.dot(vals, expo.astype(BF16), preferred_element_type=F32)
            acc_ref[yq, :, cols] = acc_ref[yq, :, cols] * shrink + term

    def at_distance(j, yq):
        below = z >= j
        above = jnp.logical_and(z + j >= nz, 2 * j < nz)

        @pl.when(jnp.logical_and(below, above))
        def _():
            tiles(yq, [lax.rem(z + nz - j, nz), lax.rem(z + j, nz)])

        @pl.when(jnp.logical_xor(below, above))
        def _():
            tiles(yq, [lax.rem(jnp.where(below, z + nz - j, z + j), nz)])

    def query_block(i):
        away = (i + 1) // 2
        return lax.rem(y + jnp.where(i % 2 == 1, away, ny - away), ny)

    def first_visits(first, last):
        def visit(i, carry):
            yq = query_block(i)

            @pl.when(i > 0)
            def _():
                begin(yq)

                @pl.when(yq > y)
                def _():
                    tiles(yq, [z])

            at_distance(1, yq)
            return carry

        if first < last:
            lax.fori_loop(first, last, visit, 0)

    def complete(first, last):
        def visit(i, carry):
            def near(j, carry):
                at_distance(j, query_block(i))
                return carry

            return lax.fori_loop(2, ring_z.steps + 1, near, carry)

        if first < last and ring_z.steps > 1:
            lax.fori_loop(first, last, visit, 0)

    begin(y)
    kpos = (z * ny + y) * rows + lax.broadcasted_iota(jnp.int32, (rows, 1), 0)
    tiles(y, [z], lambda at: kpos <= positions(y, at, width))
    sy, sz = ring_y.steps, ring_z.steps
    for k in range(1, min(sy, 2) + 1):
        ring_y.step(k)
    ring_z.step(1)
    here = min(ny, 2 * min(sy, 2) + 1)
    near_end, far_end = min(3, here), max(here, ny - 2)
    first_visits(0, near_end)
    if sz >= 2:
        ring_z.step(2)
    if sy >= 3:
        ring_y.step(3)
    first_visits(near_end, here)
    if sy >= 4:
        ring_y.step(4)
    first_visits(here, far_end)
    if sz >= 3:
        ring_z.step(3)
    shared.step(1, True)
    first_visits(far_end, ny)
    if sz >= 4:
        ring_z.step(4)

    def pooled():
        here = p_ref[...].astype(F32)
        rim = jnp.where(s > 0, halo[...].astype(F32), 0.0)
        total = jnp.concatenate([rim, here], axis=0)
        slot = t % 4
        for i in range(4):
            more = total + pltpu.roll(total, 1 << i, 0)
            total = jnp.where(i <= slot, more, total)
        span = jnp.where(slot == 0, 2, jnp.where(slot == 1, 4, jnp.where(slot == 2, 8, 16)))
        pos = s * rows + lax.broadcasted_iota(jnp.int32, (rows, 1), 0)
        count = jnp.minimum(pos + 1, span).astype(F32)
        differ = (total[RIM:] / count - here).astype(BF16)
        return (jnp.dot(differ, gw_ref[0], preferred_element_type=F32) * ps_ref[...]).astype(BF16)

    def own(block, m):
        cols = slice(m * rows, (m + 1) * rows)
        return acc_ref[block, :, cols], st_ref[block, 0:1, cols], jnp.sum(sum_ref[block, :, cols], axis=0, keepdims=True)

    def joined(a, b):
        top = jnp.maximum(a[1], b[1])
        fa, fb = jnp.exp2((a[1] - top) * factor), jnp.exp2((b[1] - top) * factor)
        return a[0] * fa + b[0] * fb, top, a[2] * fa + b[2] * fb

    def landed(d, m, k):
        return wland[d, m, k].astype(F32), sland[d, m, k, 0:1], sland[d, m, k, 1:2]

    def copies(d, m, k):
        to = dev_y((y + (1 if d == 0 else ny - 1)) % ny)
        return [
            rcopy(wbuf.at[d, m, k], wland.at[d, m, k], ms.at[d, m, k], mr.at[d, m, k], to),
            rcopy(sbuf.at[d, m, k], sland.at[d, m, k], ss.at[d, m, k], sr.at[d, m, k], to),
        ]

    done = ny
    for k in range(ny // 2):
        complete(max(ny - 3 - 2 * k, 0), done)
        done = max(ny - 3 - 2 * k, 0)
        for m in range(2):
            for d in range(2):
                n = hops(ny, d, m)
                if k >= n:
                    continue
                sign = 1 if d == 0 else -1
                block = (y + sign * (n - k)) % ny
                state = own(block, m)
                if k > 0:
                    for copy in copies(d, m, k - 1):
                        copy.wait_recv()
                    state = joined(state, landed(d, m, k - 1))
                wbuf[d, m, k] = state[0].astype(BF16)
                sbuf[d, m, k, 0:1] = state[1]
                sbuf[d, m, k, 1:2] = state[2]
                for copy in copies(d, m, k):
                    copy.start()
        if k == 0:
            hcopy.wait_recv()
            branch[:, head:] = pooled()
    for m in range(2):
        state = own(y, m)
        for d in range(2):
            n = hops(ny, d, m)
            if n > 0:
                for copy in copies(d, m, n - 1):
                    copy.wait_recv()
                state = joined(state, landed(d, m, n - 1))
        if m == 0:
            mix[...] = state[0] / state[2]
        else:
            mix[...] = mix[...] - lam_ref[0:1, 0:1] * state[0] / state[2]
    mixed = mix[...]
    mean = jnp.mean(mixed * mixed, axis=0, keepdims=True)
    normed = jnp.transpose(mixed * lax.rsqrt(mean + EPSILON)) * sub_ref[...]
    branch[:, 0:head] = normed.astype(BF16)

    outs = []
    for d in range(1, tp):
        at = pl.multiple_of(((t + d) % tp) * orows, 16)
        outs.append(rcopy(branch.at[pl.ds(at, orows)], lands.at[t], os.at[d - 1], or_.at[d - 1], others[d - 1]))
        outs[-1].start()
    lands[t] = branch[pl.ds(pl.multiple_of(t * orows, 16), orows)]
    shared.step(1, False)
    shared.step(2, False)
    shared.finish()
    for copy in outs:
        copy.wait_recv()
    at = 0
    for ref in (wo_all,):
        step = math.gcd(512, ref.shape[1])
        for low in range(0, ref.shape[1], step):
            total = None
            for i in range(tp):
                term = lax.dot_general(
                    lands[i], ref[i, low : low + step], (((1,), (1,)), ((), ())), preferred_element_type=F32
                )
                total = term if total is None else total + term
            out_ref[:, at : at + step] = total.astype(BF16)
            at += step
    for copy in outs:
        copy.wait_send()
    for k in range(ny // 2):
        for m in range(2):
            for d in range(2):
                if k < hops(ny, d, m):
                    for copy in copies(d, m, k):
                        copy.wait_send()
    hcopy.wait_send()
    ring_z.finish()
    ring_y.finish()


def local(sp, tp, tokens, pre_gain, w_query, w_key, w_value, w_pool, lambdas, sub_gain, group_weight, pool_scale, w_out):
    nz, ny = grid_of(sp)
    nx = tp // 2
    rows, part = tokens.shape
    wrows = w_query.shape[0]
    head = w_value.shape[1]
    qd = w_query.shape[1]
    whole = 3 * qd + 3 * head
    ncols = sp * w_out.shape[1]
    scale = 1.0 / math.sqrt(qd // 2)
    dma = pltpu.SemaphoreType.DMA
    half = ny // 2
    orows = rows // tp
    (out,) = call(
        functools.partial(layer_kernel, nz, ny, nx, scale),
        [
            pltpu.with_memory_space_constraint(a, pltpu.HBM)
            for a in (tokens, pre_gain.reshape(1, part), w_query, w_key, w_value, w_pool, w_out.T)
        ]
        + [
            jnp.broadcast_to(lambdas.reshape(1, 1), (8, 128)),
            sub_gain.reshape(1, head),
            group_weight,
            pool_scale.reshape(1, head),
        ],
        (sds(orows, ncols),),
        [
            VMEM((rows + 16, part), BF16),
            VMEM((wrows, whole), BF16),
            VMEM((1, part), BF16),
            VMEM((tp, rows + 16, part), BF16),
            VMEM((nz, ny, 2, wrows // 2, whole), BF16),
            VMEM((rows, tp * part), BF16),
            VMEM((rows, 128), F32),
            VMEM((rows, head), BF16),
            VMEM((ncols, 2 * head), BF16),
            VMEM((ny, qd, rows), BF16),
            VMEM((nz, rows, qd), BF16),
            VMEM((nz, head, rows), BF16),
            VMEM((RIM, head), BF16),
            VMEM((tp, ncols, 2 * head), BF16),
            VMEM((ny, head, 2 * rows), F32),
            VMEM((ny, 8, 2 * rows), F32),
            VMEM((ny, qd, 2 * rows), BF16),
            VMEM((ny, 8, 2 * rows), F32),
            VMEM((head, rows), F32),
            VMEM((rows, 2 * head), BF16),
            VMEM((2, 2, half, head, rows), BF16),
            VMEM((2, 2, half, 2, rows), F32),
            VMEM((2, 2, half, head, rows), BF16),
            VMEM((2, 2, half, 2, rows), F32),
            VMEM((tp, orows, 2 * head), BF16),
        ]
        + [dma((7,)), dma((2 * nx,)), dma((2 * nx,)), dma((ny,)), dma((ny,)), dma((nz,)), dma((nz,))]
        + ring_sems(nz, 2)
        + ring_sems(ny, 2)
        + ring_sems(nz, 2)
        + ring_sems(ny, 2)
        + shared_sems(nx, PARTS)
        + [dma, dma]
        + [dma((2, 2, half))] * 4
        + [dma((tp,))] * 2,
        cid=0,
        space=[pltpu.HBM] * 7 + [VMEM] * 4,
        name="layer",
    )
    return out


def solution(mesh):
    placed = (
        P("sp", "tp"),
        P("tp"),
        P("sp", "tp"),
        P("sp", "tp"),
        P("sp", "tp"),
        P("sp", "tp"),
        P("tp"),
        P(),
        P("tp", None, None),
        P("tp"),
        P("tp", "sp"),
    )
    body = functools.partial(local, mesh.shape["sp"], mesh.shape["tp"])
    return jax.shard_map(body, mesh=mesh, in_specs=placed, out_specs=P(("sp", "tp"), None), check_vma=False)
```

```python
import functools
import math

import jax
import jax.numpy as jnp
from jax import lax
from jax.experimental import pallas as pl
from jax.experimental.pallas import tpu as pltpu
from jax.sharding import PartitionSpec as P

MESH = pl.DeviceIdType.MESH
VMEM = pltpu.VMEM
EPSILON = 1e-06
NEG_LARGE = -1e30
F32, BF16 = jnp.float32, jnp.bfloat16
RIM = 16
LEAD = 1
PARTS = 8


def grid_of(sp):
    ny = 2 ** ((sp.bit_length() - 1) // 2)
    return sp // ny, ny


def vspec(n):
    return [pl.BlockSpec(memory_space=VMEM)] * n


def sds(*shape, dtype=BF16):
    return jax.ShapeDtypeStruct(shape, dtype)


def call(kernel, ins, outs, scratch=(), cid=None, limit=40 << 20, name=None, flops=1 << 24, space=()):
    params = dict(vmem_limit_bytes=limit)
    if cid is not None:
        params.update(collective_id=cid, has_side_effects=True)
    return pl.pallas_call(
        kernel,
        out_shape=tuple(outs),
        in_specs=[pl.BlockSpec(memory_space=one) for one in space],
        out_specs=tuple(vspec(len(outs))),
        scratch_shapes=list(scratch),
        compiler_params=pltpu.CompilerParams(**params),
        cost_estimate=pl.CostEstimate(flops=flops, bytes_accessed=1 << 20, transcendentals=0),
        name=name,
    )(*ins)


def rcopy(src, dst, ssem, rsem, dev):
    return pltpu.make_async_remote_copy(
        src_ref=src, dst_ref=dst, send_sem=ssem, recv_sem=rsem, device_id=dev, device_id_type=MESH
    )


def greet(peers):
    barrier = pltpu.get_barrier_semaphore()
    for dev in peers:
        pl.semaphore_signal(barrier, inc=1, device_id=dev, device_id_type=MESH)
    pl.semaphore_wait(barrier, len(peers))


def hops(n, direction, sub):
    return n // 2 if (direction + sub) % 2 == 0 else (n - 1) // 2


class Ring:
    def __init__(self, n, me, dev, piece, subs, ssem, rsem):
        self.n, self.me, self.dev, self.piece, self.subs = n, me, dev, piece, subs
        self.ssem, self.rsem = ssem, rsem
        self.steps = n // 2

    def copy(self, d, sub, k):
        sign = 1 if d == 0 else -1
        block = (self.me - sign * k) % self.n
        ref = self.piece(block, sub)
        return rcopy(
            ref, ref, self.ssem.at[d, sub, k], self.rsem.at[d, sub, k], self.dev((self.me + sign) % self.n)
        )

    def step(self, k):
        for sub in range(self.subs):
            for d in range(2):
                if k > 0 and k - 1 < hops(self.n, d, sub):
                    self.copy(d, sub, k - 1).wait_recv()
                if k < hops(self.n, d, sub):
                    self.copy(d, sub, k).start()

    def open(self):
        for far in range(self.steps, 0, -1):
            for sub in range(self.subs):
                for d in range(2):
                    if hops(self.n, d, sub) == far:
                        self.copy(d, sub, 0).start()

    def pass_on(self, k, landed, onward):
        for sub in range(self.subs):
            for d in range(2):
                if k - 1 < hops(self.n, d, sub) and (k < hops(self.n, d, sub)) == onward:
                    self.copy(d, sub, k - 1).wait_recv()
                    if onward:
                        self.copy(d, sub, k).start()
                    landed((self.me + (k if d else -k)) % self.n, sub)

    def finish(self):
        for k in range(self.steps):
            for sub in range(self.subs):
                for d in range(2):
                    if k < hops(self.n, d, sub):
                        self.copy(d, sub, k).wait_send()


def ring_sems(n, subs):
    return [pltpu.SemaphoreType.DMA((2, subs, max(n // 2, 1))), pltpu.SemaphoreType.DMA((2, subs, max(n // 2, 1)))]


class Shared:
    def __init__(self, nx, own, buf, subs, size, rs, rr, ps, pr):
        s, t = lax.axis_index("sp"), lax.axis_index("tp")
        x, c = t // 2, t % 2
        self.nx, self.x, self.c, self.t = nx, x, c, t
        self.buf, self.ps, self.pr, self.own = buf, ps, pr, own
        self.partner = (s, x * 2 + 1 - c)
        self.peers = [(s, ((x + d) % nx) * 2 + c) for d in ((1, nx - 1) if nx > 1 else ())] + [self.partner]
        self.piece = lambda b, i: buf.at[2 * b + c, i * size : (i + 1) * size]
        self.ring = Ring(nx, x, lambda i: (s, 2 * i + c), self.piece, subs, rs, rr)
        self.subs = subs
        self.relays = []

    def relay(self, block, sub):
        ref = self.piece(block, sub)
        at = len(self.relays)
        copy = rcopy(ref, ref, self.ps.at[at], self.pr.at[at], self.partner)
        copy.start()
        self.relays.append(copy)

    def start(self):
        self.buf[self.t] = self.own[...]
        self.ring.open()
        self.direct = rcopy(
            self.own, self.buf.at[self.t], self.ps.at[self.subs * self.nx], self.pr.at[self.subs * self.nx], self.partner
        )
        self.direct.start()

    def step(self, k, onward):
        if k <= self.ring.steps:
            self.ring.pass_on(k, self.relay, onward)

    def finish(self):
        for copy in self.relays + [self.direct]:
            copy.wait_recv()
        for copy in self.relays + [self.direct]:
            copy.wait_send()
        self.ring.finish()


def shared_sems(nx, subs):
    dma = pltpu.SemaphoreType.DMA
    return ring_sems(nx, subs) + [dma((subs * nx + 1,)), dma((subs * nx + 1,))]


def layer_kernel(
    nz, ny, nx, scale, tin_ref, gain_ref, wq_ref, wk_ref, wv_ref, wp_ref, wot_ref, lam_ref, sub_ref, gw_ref, ps_ref, out_ref,
    tok_ref, w_ref, gain, tok_full, w_full, scaled, sq, p_ref, wo_ref,
    q_all, k_all, v_all, halo, wo_all, acc_ref, st_ref, qz_ref, sum_ref, mix, branch, wbuf, sbuf, wland, sland, lands,
    ins, ts, tr, ys, yr, zs, zr, ga_s, ga_r, gb_s, gb_r,
    ks, kr, qs, qr, xs, xr, ps, pr, hs, hr, ms, mr, ss, sr, os, or_,
):
    orows = out_ref.shape[0]
    s, t = lax.axis_index("sp"), lax.axis_index("tp")
    z, y, x, c = s // ny, s % ny, t // 2, t % 2
    half = w_ref.shape[0] // 2
    rows, part = tin_ref.shape
    qd, head = wq_ref.shape[1], wv_ref.shape[1]
    sp, tp = nz * ny, 2 * nx
    loads = [pltpu.make_async_copy(tin_ref, tok_ref.at[0:rows], ins.at[0]), pltpu.make_async_copy(gain_ref, gain, ins.at[1])]
    at = 0
    for i, ref in enumerate((wq_ref, wk_ref, wv_ref, wp_ref, wot_ref)):
        loads.append(pltpu.make_async_copy(ref, w_ref.at[:, at : at + ref.shape[1]], ins.at[2 + i]))
        at += ref.shape[1]
    for load in loads:
        load.start()
    loads[1].wait()
    tok_ref[rows:] = jnp.broadcast_to(gain[...], (16, gain.shape[1]))
    partner = (s, x * 2 + 1 - c)
    across = [(s, ((x + d) % nx) * 2 + c) for d in range(1, nx)]
    along_y = [(z * ny + (y + d) % ny, t) for d in range(1, ny)]
    along_z = [(((z + d) % nz) * ny + y, t) for d in range(1, nz)]
    dev_z = lambda i: (i * ny + y, t)
    dev_y = lambda i: (z * ny + i, t)
    nxt, prv = ((s + 1) % sp, t), ((s + sp - 1) % sp, t)
    others = [(s, (t + d) % tp) for d in range(1, tp)]
    greet(others + along_y + along_z + [nxt, prv])
    for i, load in enumerate(loads):
        if i != 1:
            load.wait()

    ysends = [
        rcopy(w_ref.at[0:half], w_full.at[z, y, 0], ys.at[d], yr.at[d], along_y[d]) for d in range(ny - 1)
    ]
    zsends = [
        rcopy(w_ref.at[half:], w_full.at[z, y, 1], zs.at[d], zr.at[d], along_z[d]) for d in range(nz - 1)
    ]
    tsends = [rcopy(tok_ref, tok_full.at[t], ts.at[d], tr.at[d], across[d]) for d in range(nx - 1)]
    tsends.append(rcopy(tok_ref, tok_full.at[t], ts.at[nx - 1], tr.at[nx - 1], partner))
    for copy in ysends + zsends + tsends:
        copy.start()
    w_full[z, y, 0] = w_ref[0:half]
    w_full[z, y, 1] = w_ref[half:]
    tok_full[t] = tok_ref[...]

    def piece_a(block, sub):
        return w_full.at[block, sub * (ny // 2) : (sub + 1) * (ny // 2), 0]

    def piece_b(block, sub):
        return w_full.at[sub * (nz // 2) : (sub + 1) * (nz // 2), block, 1]

    ring_a = Ring(nz, z, lambda i: (i * ny + y, t), piece_a, 2, ga_s, ga_r)
    ring_b = Ring(ny, y, lambda i: (z * ny + i, t), piece_b, 2, gb_s, gb_r)
    for copy in ysends:
        copy.wait_recv()
    ring_a.step(0)
    for copy in zsends:
        copy.wait_recv()
    ring_b.step(0)
    relays = []
    for k in range(1, max(ring_a.steps, ring_b.steps) + 1):
        if k <= ring_a.steps:
            ring_a.step(k)
        if k <= ring_b.steps:
            ring_b.step(k)
        if k == 1:
            for d in range(nx - 1):
                tsends[d].wait_recv()
                source = ((x - 1 - d) % nx) * 2 + c
                relays.append(
                    rcopy(tok_full.at[source], tok_full.at[source], ts.at[nx + d], tr.at[nx + d], partner)
                )
                relays[-1].start()
    tsends[-1].wait_recv()
    for copy in relays:
        copy.wait_recv()
    for copy in ysends + zsends + tsends + relays:
        copy.wait_send()
    ring_a.finish()
    ring_b.finish()
    wo_ref[...] = w_full[:, :, :, :, 512:].reshape(wo_ref.shape)
    sq[...] = jnp.zeros_like(sq)
    for i in range(tp):
        values = tok_full[i, 0:rows].astype(F32)
        weight = tok_full[i, rows : rows + 1].astype(F32)
        squares = values * values
        for lane in range(0, part, 128):
            sq[...] += squares[:, lane : lane + 128]
        scaled[:, i * part : (i + 1) * part] = (values * weight).astype(BF16)
    inverse = lax.rsqrt(jnp.sum(sq[...], axis=1, keepdims=True) / (tp * part) + EPSILON)

    def project(at):
        out = jnp.dot(scaled[...], w_full[:, :, :, :, at * 128 : at * 128 + 256].reshape(tp * part, 256), preferred_element_type=F32) * inverse
        return out[:, 0:128].astype(BF16), out[:, 128:256].astype(BF16)

    q, k = project(0)
    q_all[y] = jnp.transpose(q.astype(F32)).astype(BF16)
    k_all[z] = k
    v, p = project(2)
    v_all[z] = jnp.transpose(v.astype(F32)).astype(BF16)
    p_ref[...] = p
    shared = Shared(nx, wo_ref, wo_all, PARTS, wo_ref.shape[0] // PARTS, xs, xr, ps, pr)
    half = qd // 2
    ring_y = Ring(ny, y, dev_y, lambda b, i: q_all.at[b, i * half : (i + 1) * half], 2, qs, qr)
    ring_z = Ring(nz, z, dev_z, lambda b, i: (k_all if i == 0 else v_all).at[b], 2, ks, kr)
    ring_y.step(0)
    ring_z.step(0)
    shared.start()
    hcopy = rcopy(p_ref.at[rows - RIM :], halo, hs, hr, nxt)
    hcopy.start()

    lanes = 2 * rows
    width = min(256, rows)
    vd = v_all.shape[1]
    factor = scale / math.log(2.0)

    def positions(yq, at, wide):
        lane = lax.broadcasted_iota(jnp.int32, (1, wide), 1) + at
        return jnp.where(lane >= rows, lane - rows, lane) + (z * ny + yq) * rows

    def begin(yq):
        qt = q_all[yq]
        low = lax.broadcasted_iota(jnp.int32, qt.shape, 0) < half
        zero = jnp.zeros_like(qt)
        qz_ref[yq, :, 0:rows] = jnp.where(low, qt, zero)
        qz_ref[yq, :, rows:] = jnp.where(low, zero, qt)
        acc_ref[yq] = jnp.zeros((vd, lanes), F32)
        sum_ref[yq] = jnp.zeros((8, lanes), F32)
        st_ref[yq, 0:1] = jnp.full((1, lanes), NEG_LARGE, F32)

    def tiles(yq, blocks, mask=None):
        keys = jnp.concatenate([k_all[b] for b in blocks], axis=0)
        vals = jnp.concatenate([v_all[b] for b in blocks], axis=1)
        depth = keys.shape[0]
        work = list(range(0, lanes, width))

        def scores(at):
            sc = jnp.dot(keys, qz_ref[yq, :, at : at + width], preferred_element_type=F32)
            if mask is not None:
                sc = jnp.where(mask(at), sc, NEG_LARGE)
            return sc, jnp.max(sc, axis=0, keepdims=True)

        ahead = [scores(at) for at in work[:LEAD]]
        for i, at in enumerate(work):
            sc, top = ahead.pop(0)
            if i + LEAD < len(work):
                ahead.append(scores(work[i + LEAD]))
            cols = slice(at, at + width)
            old = st_ref[yq, 0:1, cols]
            new = jnp.maximum(old, top)
            expo = jnp.exp2(sc * factor - new * factor)
            if mask is not None:
                expo = jnp.where(mask(at), expo, 0.0)
            shrink = jnp.exp2((old - new) * factor)
            st_ref[yq, 0:1, cols] = new
            part = jnp.sum(expo.reshape(depth // 8, 8, width), axis=0)
            sum_ref[yq, :, cols] = sum_ref[yq, :, cols] * shrink + part
            term = jnp.dot(vals, expo.astype(BF16), preferred_element_type=F32)
            acc_ref[yq, :, cols] = acc_ref[yq, :, cols] * shrink + term

    def at_distance(j, yq):
        below = z >= j
        above = jnp.logical_and(z + j >= nz, 2 * j < nz)

        @pl.when(jnp.logical_and(below, above))
        def _():
            tiles(yq, [lax.rem(z + nz - j, nz), lax.rem(z + j, nz)])

        @pl.when(jnp.logical_xor(below, above))
        def _():
            tiles(yq, [lax.rem(jnp.where(below, z + nz - j, z + j), nz)])

    def query_block(i):
        away = (i + 1) // 2
        return lax.rem(y + jnp.where(i % 2 == 1, away, ny - away), ny)

    def first_visits(first, last):
        def visit(i, carry):
            yq = query_block(i)

            @pl.when(i > 0)
            def _():
                begin(yq)

                @pl.when(yq > y)
                def _():
                    tiles(yq, [z])

            at_distance(1, yq)
            return carry

        if first < last:
            lax.fori_loop(first, last, visit, 0)

    def complete(first, last):
        def visit(i, carry):
            def near(j, carry):
                at_distance(j, query_block(i))
                return carry

            return lax.fori_loop(2, ring_z.steps + 1, near, carry)

        if first < last and ring_z.steps > 1:
            lax.fori_loop(first, last, visit, 0)

    begin(y)
    kpos = (z * ny + y) * rows + lax.broadcasted_iota(jnp.int32, (rows, 1), 0)
    tiles(y, [z], lambda at: kpos <= positions(y, at, width))
    sy, sz = ring_y.steps, ring_z.steps
    ring_y.step(1)
    ring_z.step(1)
    if sy >= 2:
        ring_y.step(2)
    here = min(ny, 2 * min(sy, 2) + 1)
    near_end, far_end = min(3, here), max(here, ny - 2)
    first_visits(0, near_end)
    if sz >= 2:
        ring_z.step(2)
    if sy >= 3:
        ring_y.step(3)
    first_visits(near_end, here)
    if sy >= 4:
        ring_y.step(4)
    first_visits(here, far_end)
    if sz >= 3:
        ring_z.step(3)
    shared.step(1, True)
    first_visits(far_end, ny)
    if sz >= 4:
        ring_z.step(4)

    def pooled():
        here = p_ref[...].astype(F32)
        rim = jnp.where(s > 0, halo[...].astype(F32), 0.0)
        total = jnp.concatenate([rim, here], axis=0)
        slot = t % 4
        for i in range(4):
            more = total + pltpu.roll(total, 1 << i, 0)
            total = jnp.where(i <= slot, more, total)
        span = jnp.where(slot == 0, 2, jnp.where(slot == 1, 4, jnp.where(slot == 2, 8, 16)))
        pos = s * rows + lax.broadcasted_iota(jnp.int32, (rows, 1), 0)
        count = jnp.minimum(pos + 1, span).astype(F32)
        differ = (total[RIM:] / count - here).astype(BF16)
        return (jnp.dot(differ, gw_ref[0], preferred_element_type=F32) * ps_ref[...]).astype(BF16)

    def own(block, m):
        cols = slice(m * rows, (m + 1) * rows)
        return acc_ref[block, :, cols], st_ref[block, 0:1, cols], jnp.sum(sum_ref[block, :, cols], axis=0, keepdims=True)

    def joined(a, b):
        top = jnp.maximum(a[1], b[1])
        fa, fb = jnp.exp2((a[1] - top) * factor), jnp.exp2((b[1] - top) * factor)
        return a[0] * fa + b[0] * fb, top, a[2] * fa + b[2] * fb

    def landed(d, m, k):
        return wland[d, m, k].astype(F32), sland[d, m, k, 0:1], sland[d, m, k, 1:2]

    def copies(d, m, k):
        to = dev_y((y + (1 if d == 0 else ny - 1)) % ny)
        return [
            rcopy(wbuf.at[d, m, k], wland.at[d, m, k], ms.at[d, m, k], mr.at[d, m, k], to),
            rcopy(sbuf.at[d, m, k], sland.at[d, m, k], ss.at[d, m, k], sr.at[d, m, k], to),
        ]

    done = ny
    for k in range(ny // 2):
        complete(max(ny - 3 - 2 * k, 0), done)
        done = max(ny - 3 - 2 * k, 0)
        for m in range(2):
            for d in range(2):
                n = hops(ny, d, m)
                if k >= n:
                    continue
                sign = 1 if d == 0 else -1
                block = (y + sign * (n - k)) % ny
                state = own(block, m)
                if k > 0:
                    for copy in copies(d, m, k - 1):
                        copy.wait_recv()
                    state = joined(state, landed(d, m, k - 1))
                wbuf[d, m, k] = state[0].astype(BF16)
                sbuf[d, m, k, 0:1] = state[1]
                sbuf[d, m, k, 1:2] = state[2]
                for copy in copies(d, m, k):
                    copy.start()
        if k == 0:
            hcopy.wait_recv()
            branch[:, head:] = pooled()
    for m in range(2):
        state = own(y, m)
        for d in range(2):
            n = hops(ny, d, m)
            if n > 0:
                for copy in copies(d, m, n - 1):
                    copy.wait_recv()
                state = joined(state, landed(d, m, n - 1))
        if m == 0:
            mix[...] = state[0] / state[2]
        else:
            mix[...] = mix[...] - lam_ref[0:1, 0:1] * state[0] / state[2]
    mixed = mix[...]
    mean = jnp.mean(mixed * mixed, axis=0, keepdims=True)
    normed = jnp.transpose(mixed * lax.rsqrt(mean + EPSILON)) * sub_ref[...]
    branch[:, 0:head] = normed.astype(BF16)

    outs = []
    for d in range(1, tp):
        at = pl.multiple_of(((t + d) % tp) * orows, 16)
        outs.append(rcopy(branch.at[pl.ds(at, orows)], lands.at[t], os.at[d - 1], or_.at[d - 1], others[d - 1]))
        outs[-1].start()
    lands[t] = branch[pl.ds(pl.multiple_of(t * orows, 16), orows)]
    shared.step(1, False)
    shared.step(2, False)
    shared.finish()
    for copy in outs:
        copy.wait_recv()
    at = 0
    for ref in (wo_all,):
        step = math.gcd(512, ref.shape[1])
        for low in range(0, ref.shape[1], step):
            total = None
            for i in range(tp):
                term = lax.dot_general(
                    lands[i], ref[i, low : low + step], (((1,), (1,)), ((), ())), preferred_element_type=F32
                )
                total = term if total is None else total + term
            out_ref[:, at : at + step] = total.astype(BF16)
            at += step
    for copy in outs:
        copy.wait_send()
    for k in range(ny // 2):
        for m in range(2):
            for d in range(2):
                if k < hops(ny, d, m):
                    for copy in copies(d, m, k):
                        copy.wait_send()
    hcopy.wait_send()
    ring_z.finish()
    ring_y.finish()


def local(sp, tp, tokens, pre_gain, w_query, w_key, w_value, w_pool, lambdas, sub_gain, group_weight, pool_scale, w_out):
    nz, ny = grid_of(sp)
    nx = tp // 2
    rows, part = tokens.shape
    wrows = w_query.shape[0]
    head = w_value.shape[1]
    qd = w_query.shape[1]
    whole = 3 * qd + 3 * head
    ncols = sp * w_out.shape[1]
    scale = 1.0 / math.sqrt(qd // 2)
    dma = pltpu.SemaphoreType.DMA
    half = ny // 2
    orows = rows // tp
    (out,) = call(
        functools.partial(layer_kernel, nz, ny, nx, scale),
        [
            pltpu.with_memory_space_constraint(a, pltpu.HBM)
            for a in (tokens, pre_gain.reshape(1, part), w_query, w_key, w_value, w_pool, w_out.T)
        ]
        + [
            jnp.broadcast_to(lambdas.reshape(1, 1), (8, 128)),
            sub_gain.reshape(1, head),
            group_weight,
            pool_scale.reshape(1, head),
        ],
        (sds(orows, ncols),),
        [
            VMEM((rows + 16, part), BF16),
            VMEM((wrows, whole), BF16),
            VMEM((1, part), BF16),
            VMEM((tp, rows + 16, part), BF16),
            VMEM((nz, ny, 2, wrows // 2, whole), BF16),
            VMEM((rows, tp * part), BF16),
            VMEM((rows, 128), F32),
            VMEM((rows, head), BF16),
            VMEM((ncols, 2 * head), BF16),
            VMEM((ny, qd, rows), BF16),
            VMEM((nz, rows, qd), BF16),
            VMEM((nz, head, rows), BF16),
            VMEM((RIM, head), BF16),
            VMEM((tp, ncols, 2 * head), BF16),
            VMEM((ny, head, 2 * rows), F32),
            VMEM((ny, 8, 2 * rows), F32),
            VMEM((ny, qd, 2 * rows), BF16),
            VMEM((ny, 8, 2 * rows), F32),
            VMEM((head, rows), F32),
            VMEM((rows, 2 * head), BF16),
            VMEM((2, 2, half, head, rows), BF16),
            VMEM((2, 2, half, 2, rows), F32),
            VMEM((2, 2, half, head, rows), BF16),
            VMEM((2, 2, half, 2, rows), F32),
            VMEM((tp, orows, 2 * head), BF16),
        ]
        + [dma((7,)), dma((2 * nx,)), dma((2 * nx,)), dma((ny,)), dma((ny,)), dma((nz,)), dma((nz,))]
        + ring_sems(nz, 2)
        + ring_sems(ny, 2)
        + ring_sems(nz, 2)
        + ring_sems(ny, 2)
        + shared_sems(nx, PARTS)
        + [dma, dma]
        + [dma((2, 2, half))] * 4
        + [dma((tp,))] * 2,
        cid=0,
        space=[pltpu.HBM] * 7 + [VMEM] * 4,
        name="layer",
    )
    return out


def solution(mesh):
    placed = (
        P("sp", "tp"),
        P("tp"),
        P("sp", "tp"),
        P("sp", "tp"),
        P("sp", "tp"),
        P("sp", "tp"),
        P("tp"),
        P(),
        P("tp", None, None),
        P("tp"),
        P("tp", "sp"),
    )
    body = functools.partial(local, mesh.shape["sp"], mesh.shape["tp"])
    return jax.shard_map(body, mesh=mesh, in_specs=placed, out_specs=P(("sp", "tp"), None), check_vma=False)
```
